32 devices in a mesh: sp: 16 (over z, y, x), tp: 2 (over core).
Axes of the slice: x: 2, y: 2, z: 4, core: 2. Of those that a mesh axis runs over, the one named last changes fastest.
Arguments:
- stream: bfloat16 [4096, 2048], P(('sp', 'tp')), may hold values from -6 to 6
- outer_gate: bfloat16 [4096, 1024], P('sp', 'tp'), may hold values from -6 to 6
- inner_gate: bfloat16 [4096, 1024], P('sp', 'tp'), may hold values from -6 to 6
- conv_values: bfloat16 [4096, 1024], P('sp', 'tp'), may hold values from -6 to 6
- doc_ids: int32 [4096], P('sp'), may hold values from 0 to 7, never falling along the last dimension, each value on 1 to 1024 neighbouring positions
- conv_taps: float32 [3, 1024], P(None, 'tp'), may hold values from -3.5 to 3.5
- out_weight: bfloat16 [1024, 2048], replicated, may hold values from -0.1875 to 0.1875
- norm_gain: float32 [2048], replicated, may hold values from 0.1 to 1.9
- route_ids: int32 [4096, 2], P(('sp', 'tp')), may hold values from 0 to 31, all different within a row; in each aligned block of 128 rows (0 to 127, 128 to 255, ...) at most 16 rows name the same one
- route_logits: float32 [4096, 2], P(('sp', 'tp')), may hold values from -4 to 4
- group_weight: float32 [4096], P(('sp', 'tp')), may hold values from 0.25 to 1
- w_gate: bfloat16 [32, 2048, 1024], P(('sp', 'tp')), may hold values from -0.125 to 0.125
- w_up: bfloat16 [32, 2048, 1024], P(('sp', 'tp')), may hold values from -0.125 to 0.125
- w_down: bfloat16 [32, 1024, 2048], P(('sp', 'tp')), may hold values from -0.1875 to 0.1875
Outputs:
- result: bfloat16 [4096, 2048], P(('sp', 'tp'))
The draws below stay inside these ranges and needn't reach their ends.
Inputs may be any that keep to these rules, and one draw needn't show every extreme that they name: `route_ids`: the two experts of a token differ. In the rows of one device (aligned blocks of 128 rows) no expert is named more than 16 times, a bound that some block reaches. `doc_ids`: document numbers never fall along the sequence; a document has 1 to 1024 positions and one has exactly 1024.
All inputs are finite; a program needn't handle non-finite values.
Results may differ from the reference program's by a relative error of at most 0.0052.
Values may be sent and summed in bfloat16 or wider, within the bound.
A program may use at most 64 MiB of HBM per device.

```python
import math
import jax
import jax.numpy as jnp
import numpy as np
from jax import lax

D = 2048
CW = 1024
FF = 1024
TOPK = 2
ROWS = 128
TOKENS = 4096
EXPERTS = 32
CAP = 16
DOCS = 8
MOST_DOC = 1024


def levels(key, shape, cuts, least, high):
    def one(axis_at, shards_of):
        steps = jax.random.uniform(jax.random.fold_in(jax.random.fold_in(key, 6), axis_at), (shards_of,), jnp.float32, least / len(cuts), high / len(cuts))
        return jnp.repeat(jnp.exp(steps), shape[axis_at] // shards_of).reshape((-1,) + (1,) * (len(shape) - axis_at - 1))

    level = one(*cuts[0])
    for cut in cuts[1:]:
        level = level * one(*cut)
    return level


def length_profile(number_of, total, limit, lean):
    portions = [(1 << 20) // math.isqrt(grade ** lean) + 1 for grade in range(2, number_of + 1)]
    surplus, given = total - limit - (number_of - 1), [1] * (number_of - 1)
    while surplus > 0:
        movable = [i for i in range(number_of - 1) if given[i] < limit]
        mass, budget = sum([portions[i] for i in movable]), surplus
        for i in movable:
            extra = min(limit - given[i], max(1, budget * portions[i] // mass), surplus)
            given[i] = given[i] + extra
            surplus = surplus - extra
    return np.array([limit] + given)


def ragged(stream_key, count, total, bound, lean):
    if count == 2:
        one = jax.random.randint(stream_key, (), max(1, total - bound), min(bound, total - 1) + 1)
        return jnp.stack([one, total - one])
    tallies = jnp.asarray(length_profile(count, total, bound, lean), jnp.int32)
    twos = (count - 1) // 2
    giver, taker = tallies[1:1 + 2 * twos:2], tallies[2:2 + 2 * twos:2]
    margin = jnp.minimum(giver - 1, bound - taker)
    passed = jax.random.randint(jax.random.fold_in(stream_key, 1), (twos,), 0, 1 << 20) % (margin + 1)
    tallies = tallies.at[1:1 + 2 * twos:2].set(giver - passed).at[2:2 + 2 * twos:2].set(taker + passed)
    return tallies[jax.random.permutation(jax.random.fold_in(stream_key, 2), count)]


def routed_block(rng, own, number, rows, amount, top, bound, slope):
    sequence = jax.random.permutation(rng, amount)
    packed, ordinary = portions_of(amount, rows * top, bound, slope, True), portions_of(amount, rows * top, bound, slope, False)
    places = jnp.arange(amount)

    def named(sizes, turn):
        used = int((sizes > 0).sum())
        fixed = max(1, used // 4)
        passed = fixed + (places - fixed + turn * (used - fixed)) % max(1, amount - fixed)
        return jnp.zeros((amount,), jnp.int32).at[sequence[jnp.where(places < fixed, places, passed)]].set(jnp.asarray(sizes, jnp.int32))

    sizes = jnp.where(number % 4 == 0, named(packed, number // 4), named(ordinary, number - number // 4 - 1))
    mixed = jax.random.permutation(jax.random.fold_in(own, 3), amount)
    donor, taker = mixed[0:amount // 2 * 2:2], mixed[1:amount // 2 * 2:2]
    slack = jnp.minimum(sizes[donor] - 1, bound - sizes[taker]) // 2
    slack = jnp.where((donor == sequence[0]) | (taker == sequence[0]) | (sizes[taker] == 0), 0, jnp.maximum(slack, 0))
    passed = jax.random.randint(jax.random.fold_in(own, 4), (amount // 2,), 0, 1 << 20) % (slack + 1)
    sizes = sizes.at[donor].add(-passed).at[taker].add(passed)
    members = jnp.searchsorted(jnp.cumsum(sizes), jnp.arange(rows * top), side="right").astype(jnp.int32)
    grid = members.reshape(top, rows).T
    grid = grid[jax.random.permutation(jax.random.fold_in(own, 1), rows)]
    turn = jax.random.randint(jax.random.fold_in(own, 2), (rows, 1), 0, top)
    return jnp.take_along_axis(grid, (jnp.arange(top)[None, :] + turn) % top, axis=1)


def portions_of(count, total, bound, lean, full):
    loads = [(1 << 20) // math.isqrt(rank ** lean) + 1 for rank in range(1, count + 1)]
    largest = bound if full else min(bound, max(-(-total // count), total * loads[0] // sum(loads)))
    least = 1 if total - largest >= count - 1 else 0
    counts, surplus = [largest] + [least] * (count - 1), total - largest - least * (count - 1)
    while surplus > 0:
        candidates = [i for i in range(1, count) if counts[i] < largest] or [i for i in range(1, count) if counts[i] < bound]
        mass, remaining = sum([loads[i] for i in candidates]), surplus
        for i in candidates:
            extra = min(bound - counts[i], max(1, remaining * loads[i] // mass), surplus)
            counts[i] = counts[i] + extra
            surplus = surplus - extra
    return np.array(counts)


def noise(stream_key, dims, deviation, bound, pieces=(), held_as=jnp.bfloat16):
    result = jax.random.normal(stream_key, dims, jnp.float32) * deviation
    if len(pieces) > 0:
        result = levels(stream_key, dims, pieces, -0.22, 0.18) * result
    return jnp.clip(result, min=-bound, max=bound).astype(held_as)


def setup_inputs(seed: int = 0) -> dict:
    arg_keys = jax.random.split(jax.random.key(seed), 15)
    stream = noise(arg_keys[0], (TOKENS, D), 1.0, 6.0, ((0, 32),))
    outer_gate = noise(arg_keys[1], (TOKENS, CW), 1.0, 6.0, ((0, 16), (1, 2)))
    inner_gate = noise(arg_keys[2], (TOKENS, CW), 1.0, 6.0, ((0, 16), (1, 2)))
    conv_values = noise(arg_keys[3], (TOKENS, CW), 1.0, 6.0, ((0, 16), (1, 2)))
    doc_ids = jnp.searchsorted(jnp.cumsum(ragged(arg_keys[4], DOCS, TOKENS, MOST_DOC, 1)), jnp.arange(TOKENS), side="right").astype(jnp.int32)
    conv_taps = noise(arg_keys[5], (3, CW), 3 ** -0.5, 3.5, ((1, 2),), jnp.float32)
    out_weight = noise(arg_keys[6], (CW, D), CW ** -0.5, 0.1875)
    norm_gain = jnp.clip(1.0 + 0.18 * jax.random.normal(arg_keys[7], (D,), jnp.float32), 0.1, 1.9)
    route_ids_keys = jax.random.split(jax.random.fold_in(arg_keys[8], 1), TOKENS // ROWS)
    route_ids_turns = jax.random.permutation(jax.random.fold_in(arg_keys[8], 3), TOKENS // ROWS)
    route_ids = jax.vmap(lambda own, number: routed_block(jax.random.fold_in(arg_keys[8], 2), own, number, ROWS, EXPERTS, TOPK, CAP, 2))(route_ids_keys, route_ids_turns).reshape((TOKENS, TOPK))
    route_logits = noise(arg_keys[9], (TOKENS, TOPK), 1.5, 4.0, ((0, 32),), jnp.float32)
    group_weight = jnp.clip(jnp.exp(math.log(1.0) - 1.3862944 * jax.random.uniform(arg_keys[10], (TOKENS,), jnp.float32) ** levels(arg_keys[10], (TOKENS,), ((0, 32),), -0.2, 0.2)), 0.25, 1.0)
    w_gate = noise(arg_keys[11], (EXPERTS, D, FF), D ** -0.5, 0.125, ((0, 32),))
    w_up = noise(arg_keys[12], (EXPERTS, D, FF), D ** -0.5, 0.125, ((0, 32),))
    w_down = noise(arg_keys[13], (EXPERTS, FF, D), FF ** -0.5, 0.1875, ((0, 32),))
    return {"stream": stream, "outer_gate": outer_gate, "inner_gate": inner_gate, "conv_values": conv_values, "doc_ids": doc_ids, "conv_taps": conv_taps, "out_weight": out_weight, "norm_gain": norm_gain, "route_ids": route_ids, "route_logits": route_logits, "group_weight": group_weight, "w_gate": w_gate, "w_up": w_up, "w_down": w_down}


def reference(stream, outer_gate, inner_gate, conv_values, doc_ids, conv_taps, out_weight, norm_gain, route_ids, route_logits, group_weight, w_gate, w_up, w_down):
    product = (inner_gate.astype(jnp.float32) * conv_values.astype(jnp.float32)).astype(jnp.bfloat16)
    prod_f = product.astype(jnp.float32)
    padded = jnp.pad(prod_f, ((1, 1), (0, 0)))
    padded_docs = jnp.pad(doc_ids, (1, 1), constant_values=-1)
    same_prev = (padded_docs[:-2] == doc_ids).astype(jnp.float32)[:, None]
    same_next = (padded_docs[2:] == doc_ids).astype(jnp.float32)[:, None]
    conv = conv_taps[0] * padded[:-2] * same_prev + conv_taps[1] * prod_f + conv_taps[2] * padded[2:] * same_next
    mixed = (outer_gate.astype(jnp.float32) * conv).astype(jnp.bfloat16)
    resid = stream.astype(jnp.float32) + jnp.dot(mixed, out_weight, preferred_element_type=jnp.float32)
    scale = lax.rsqrt(lax.optimization_barrier(jnp.mean(resid * resid, axis=-1, keepdims=True)) + 1e-06)
    normed = (resid * scale * norm_gain).astype(jnp.bfloat16)
    expo = jnp.exp(route_logits)
    gate = group_weight[:, None] * expo / lax.optimization_barrier(jnp.sum(expo, axis=1, keepdims=True))
    flat_ids = route_ids.reshape(-1)
    gate_flat = gate.reshape(-1)
    load = EXPERTS * CAP
    count_all = flat_ids.shape[0]

    def step(total, expert):
        is_hit = flat_ids == expert
        rank = jnp.cumsum(is_hit.astype(jnp.int32)) - 1
        where_to = jnp.where(is_hit, rank, load).astype(jnp.int32)
        pick = jnp.zeros((load,), jnp.int32).at[where_to].set(jnp.arange(count_all, dtype=jnp.int32), mode='drop')
        is_live = jnp.zeros((load,), gate_flat.dtype).at[where_to].set(1.0, mode='drop')
        token_of = pick // TOPK
        rows_in = normed[token_of]
        hidden = (jax.nn.silu(jnp.dot(rows_in, w_gate[expert], preferred_element_type=jnp.float32)) * jnp.dot(rows_in, w_up[expert], preferred_element_type=jnp.float32)).astype(jnp.bfloat16)
        expert_out = jnp.dot(hidden, w_down[expert], preferred_element_type=jnp.float32).astype(jnp.bfloat16)
        weights = gate_flat[pick] * is_live
        total = total.at[token_of].add(expert_out.astype(jnp.float32) * weights[:, None])
        return (total, None)
    total, unused = lax.scan(step, resid, jnp.arange(EXPERTS, dtype=jnp.int32))
    return total.astype(jnp.bfloat16)
```

```python
import functools

import jax
import jax.numpy as jnp
from jax import lax
from jax.experimental import pallas as pl
from jax.experimental.pallas import tpu as pltpu
from jax.sharding import PartitionSpec as P


def padded_2(shard, sides, width):
    for axis, dim in sides:
        size, length = (lax.axis_size(axis), shard.shape[dim])
        up = [(i, (i + 1) % size) for i in range(size - 1)]
        down = [(j, i) for i, j in up]
        last = lax.slice_in_dim(shard, length - width, length, axis=dim)
        leading = lax.slice_in_dim(shard, 0, width, axis=dim)
        before = lax.ppermute(last, axis, up)
        after = lax.ppermute(leading, axis, down)
        shard = jnp.concatenate([before, shard, after], axis=dim)
    return shard


def on_device(
    stream,
    outer_gate,
    inner_gate,
    conv_values,
    doc_ids,
    conv_taps,
    out_weight,
    norm_gain,
    route_ids,
    route_logits,
    group_weight,
    w_gate,
    w_up,
    w_down,
):
    tok_rows = stream.shape[0]
    width = stream.shape[1]
    product = (inner_gate.astype(jnp.float32) * conv_values.astype(jnp.float32)).astype(
        jnp.bfloat16
    )
    doc_float = doc_ids.astype(jnp.bfloat16)
    padded, padded_docs = (padded_2(product, (("sp", 0),), 1), padded_2(doc_float, (("sp", 0),), 1))
    same_prev = (padded_docs[:-2] == doc_float).astype(jnp.float32)[:, None]
    same_next = (padded_docs[2:] == doc_float).astype(jnp.float32)[:, None]
    conv = (
        conv_taps[0] * padded[:-2].astype(jnp.float32) * same_prev
        + conv_taps[1] * product.astype(jnp.float32)
        + conv_taps[2] * padded[2:].astype(jnp.float32) * same_next
    )
    mixed = (outer_gate.astype(jnp.float32) * conv).astype(jnp.bfloat16)
    channels = lax.all_to_all(mixed, "tp", split_axis=0, concat_axis=1, tiled=True)
    projected = jnp.dot(channels, out_weight, preferred_element_type=jnp.float32)
    resid = stream.astype(jnp.float32) + projected
    scale = lax.rsqrt(jnp.mean(resid * resid, axis=-1, keepdims=True) + 1e-06)
    normed = (resid * scale * norm_gain).astype(jnp.bfloat16)
    expert_total = lax.axis_size("sp") * lax.axis_size("tp")
    top_count = route_ids.shape[1]
    capacity = 2 * tok_rows * top_count // expert_total
    flat_ids = route_ids.reshape(-1)
    one_hot = (flat_ids[:, None] == jnp.arange(expert_total, dtype=jnp.int32)[None, :]).astype(
        jnp.int32
    )
    rank = jnp.sum((jnp.cumsum(one_hot, axis=0) - 1) * one_hot, axis=1)
    slot = flat_ids * capacity + rank
    slot_count = expert_total * capacity
    source_row = (
        jnp.zeros((slot_count,), jnp.int32)
        .at[slot]
        .set(jnp.arange(flat_ids.shape[0], dtype=jnp.int32) // top_count)
    )
    filled = jnp.zeros((slot_count,), jnp.bool_).at[slot].set(True)
    outgoing = jnp.where(filled[:, None], normed[source_row], jnp.zeros((), jnp.bfloat16)).reshape(
        expert_total, capacity, width
    )
    arrived = lax.all_to_all(outgoing, ("sp", "tp"), split_axis=0, concat_axis=0, tiled=True)
    sources, items, features = arrived.shape
    rows_in = arrived.reshape(sources * items, features)
    hidden = (
        jax.nn.silu(jnp.dot(rows_in, w_gate[0], preferred_element_type=jnp.float32))
        * jnp.dot(rows_in, w_up[0], preferred_element_type=jnp.float32)
    ).astype(jnp.bfloat16)
    outputs = jnp.dot(hidden, w_down[0], preferred_element_type=jnp.float32).astype(jnp.bfloat16)
    returned = lax.all_to_all(
        outputs.reshape(sources, items, features),
        ("sp", "tp"),
        split_axis=0,
        concat_axis=0,
        tiled=True,
    )
    picked = (
        returned.reshape(slot_count, width)[slot]
        .astype(jnp.float32)
        .reshape(tok_rows, top_count, width)
    )
    expo = jnp.exp(route_logits)
    gate = group_weight[:, None] * expo / jnp.sum(expo, axis=1, keepdims=True)
    result = resid + jnp.sum(gate[:, :, None] * picked, axis=1)
    return result.astype(jnp.bfloat16)


MESH = pl.DeviceIdType.MESH
F32, BF16 = jnp.float32, jnp.bfloat16


def dot(a, b):
    return jnp.dot(a, b, preferred_element_type=F32)


PARTS = 4


def fused_kernel(
    tp_size, planes, per_plane, cap,
    stream, outer, inner, values, docs, taps, gain, ids, logits, weight,
    ow_hbm, wg_hbm, wu_hbm, wd_hbm,
    out,
    ow, wg, wu, wd, edge_out, edge_in, doc_in, mix, mix_in, resid,
    meta, block, send, recv, outb, ret, acc_gate, acc_up, hidden, local, part_out, part_in,
    load_sem, edge_send, edge_recv, mix_send, mix_recv, meta_send, meta_recv,
    in_send, out_send, hop_recv, disp_send, disp_recv, back_send, back_recv,
    part_send, part_recv,
):
    sp, tp = lax.axis_index("sp"), lax.axis_index("tp")
    sp_size = planes * per_plane // tp_size
    total = planes * per_plane
    me = sp * tp_size + tp
    z, p = me // per_plane, me % per_plane
    rows, width = stream.shape
    chan = inner.shape[1]
    length = inner.shape[0]
    tile = width // PARTS
    top = ids.shape[0]
    ff = hidden.shape[1]

    middle = (z % 3 + 1) // 2
    is_middle, is_end = middle == 1, middle == 0
    step = 1 - 2 * (z // 2)
    order = [z, z + step * (1 - 2 * middle), z + step * (3 - middle), z + step * (2 - middle)]

    def place(index):
        return (index // tp_size, index % tp_size)

    inward = place((z + step) * per_plane + p)
    outward = place((z - step) * per_plane + p)

    def remote(src, dst, source_sem, target_sem, device):
        return pltpu.make_async_remote_copy(
            src_ref=src, dst_ref=dst, send_sem=source_sem, recv_sem=target_sem,
            device_id=device, device_id_type=MESH,
        )

    def wait_for(ref, sem):
        pltpu.make_async_copy(ref, ref, sem).wait()

    loads = [
        pltpu.make_async_copy(src, dst, load_sem.at[i])
        for i, (src, dst) in enumerate(
            ((ow_hbm, ow), (wg_hbm.at[0], wg), (wu_hbm.at[0], wu), (wd_hbm.at[0], wd))
        )
    ]
    for load in loads:
        load.start()

    barrier = pltpu.get_barrier_semaphore()

    def greet(i, carry):
        pl.semaphore_signal(
            barrier, inc=1, device_id=place((me + i) % total), device_id_type=MESH
        )
        return carry

    lax.fori_loop(1, total, greet, 0)
    product = (inner[...].astype(F32) * values[...].astype(F32)).astype(BF16)
    edge_out[0] = product[:16]
    edge_out[1] = product[length - 16 :]
    expo = jnp.exp(logits[...])
    gates = weight[...] * expo / jnp.sum(expo, axis=0, keepdims=True)
    meta[z] = jnp.concatenate([ids[...].astype(F32), gates, ids[...].astype(F32), gates], axis=0)
    pl.semaphore_wait(barrier, total - 1)

    left, right = ((sp + sp_size - 1) % sp_size, tp), ((sp + 1) % sp_size, tp)
    edges = []
    for side, (dest, src) in enumerate(((right, edge_out.at[1]), (left, edge_out.at[0]))):
        for kind, (source, target) in enumerate(
            ((src, edge_in.at[side]), (docs, doc_in.at[side]))
        ):
            at = 2 * side + kind
            edges.append(remote(source, target, edge_send.at[at], edge_recv.at[at], dest))
    for edge in edges:
        edge.start()

    metas = []
    for d in range(1, planes):
        there = place((z + d) % planes * per_plane + p)
        metas.append(remote(meta.at[z], meta.at[z], meta_send.at[d - 1], meta_recv.at[z], there))
    for copy in metas:
        copy.start()

    before = (
        lax.broadcasted_iota(jnp.int32, (rows, rows), 0)
        < lax.broadcasted_iota(jnp.int32, (rows, rows), 1)
    ).astype(F32).astype(BF16)
    rank_of = lax.broadcasted_iota(jnp.int32, (per_plane, cap, rows), 1).astype(F32)
    expert = (
        lax.broadcasted_iota(jnp.int32, (per_plane, rows), 0) + z * per_plane
    ).astype(F32)

    def slots(i):
        table = meta[order[i]]
        hits = [(table[k : k + 1] == expert).astype(F32) for k in range(top)]
        named = sum(hits)
        ahead = dot(named.astype(BF16), before)

        def spread(hit):
            at = jnp.where(hit > 0, ahead, -1.0)
            grid = jnp.broadcast_to(at[:, None, :], (per_plane, cap, rows))
            return jnp.where(grid == rank_of, 1.0, 0.0).reshape(per_plane * cap, rows)

        return named, hits, spread

    def to_slots(i):
        named, _, spread = slots(i)
        return spread(named).astype(BF16)

    def from_slots(i):
        _, hits, spread = slots(i)
        return [jnp.transpose(spread(hit)).astype(BF16) for hit in hits]

    def gate_columns(i):
        table = meta[order[i]]
        return [
            jnp.transpose(jnp.broadcast_to(table[top + k : top + k + 1], (rows, rows)))[:, :1]
            for k in range(top)
        ]

    picks = [to_slots(0)]

    for edge in edges:
        edge.wait()

    doc = jnp.broadcast_to(docs[...], (8, length))
    lane = lax.broadcasted_iota(jnp.int32, (8, length), 1)
    prior = jnp.where(
        lane == 0,
        pltpu.roll(jnp.broadcast_to(doc_in[0], (8, length)), 1, axis=1),
        pltpu.roll(doc, 1, axis=1),
    )
    later = jnp.where(
        lane == length - 1,
        pltpu.roll(jnp.broadcast_to(doc_in[1], (8, length)), length - 1, axis=1),
        pltpu.roll(doc, length - 1, axis=1),
    )
    spot = lane + sp * length
    same_prev = jnp.where((prior == doc) & (spot > 0), 1.0, 0.0)
    same_next = jnp.where((later == doc) & (spot < sp_size * length - 1), 1.0, 0.0)

    def column(row):
        return jnp.transpose(jnp.broadcast_to(row[:1], (128, length)))[:, :1]

    prod = product.astype(F32)
    row_at = lax.broadcasted_iota(jnp.int32, (length, chan), 0)
    prev = jnp.where(row_at == 0, edge_in[0].astype(F32)[15:16], pltpu.roll(prod, 1, axis=0))
    nxt = jnp.where(
        row_at == length - 1,
        edge_in[1].astype(F32)[:1],
        pltpu.roll(prod, length - 1, axis=0),
    )
    conv = (
        taps[0:1] * prev * column(same_prev)
        + taps[1:2] * prod
        + taps[2:3] * nxt * column(same_next)
    )
    mixed = (outer[...].astype(F32) * conv).astype(BF16)
    mix[...] = mixed.reshape(tp_size, rows, chan)
    other = 1 - tp
    swap = remote(mix.at[other], mix_in, mix_send, mix_recv, (sp, other))
    swap.start()
    loads[0].wait()
    own = mix[tp]
    for c in range(PARTS):
        cols = slice(c * tile, (c + 1) * tile)
        resid[c] = stream[:, cols].astype(F32) + dot(
            own, ow[pl.ds(pl.multiple_of(tp * chan, chan), chan), cols]
        )
    swap.wait()
    theirs = mix_in[...]
    squares = jnp.zeros((rows, 1), F32)
    for c in range(PARTS):
        cols = slice(c * tile, (c + 1) * tile)
        part = resid[c] + dot(
            theirs, ow[pl.ds(pl.multiple_of(other * chan, chan), chan), cols]
        )
        resid[c] = part
        squares = squares + jnp.sum(part * part, axis=1, keepdims=True)
    scale = lax.rsqrt(squares / width + 1e-06)

    def hop(j, c, sem, device):
        return remote(block.at[j, c], block.at[j, c], sem, hop_recv.at[j, c], device)

    def own_in(c):
        return hop(z, c, in_send.at[0, c], inward)

    def own_out(c):
        return hop(z, c, out_send.at[0, c], outward)

    def onward(i, c):
        if i == 1:
            return hop(order[1], c, in_send.at[1, c], inward)
        return hop(order[i], c, out_send.at[i - 1, c], outward)

    def forward(i, c):
        @pl.when(is_middle)
        def _():
            wait_for(block.at[order[i], c], hop_recv.at[order[i], c])
            onward(i, c).start()

    def group(src, dst, source_sem, target_sem):
        def one(i, carry):
            peer = (p + i) % per_plane
            remote(
                src.at[peer], dst.at[p], source_sem, target_sem, place(z * per_plane + peer)
            ).start()
            return carry

        lax.fori_loop(1, per_plane, one, 0)

    def wait_group(buf, sem):
        wait_for(buf.at[pl.ds(0, per_plane - 1)], sem)

    def dispatch(i, c):
        if i > 0:

            @pl.when(is_end)
            def _():
                wait_for(block.at[order[i], c], hop_recv.at[order[i], c])

        send[i, c] = (
            dot(picks[i], block[order[i], c]).astype(BF16).reshape(per_plane, cap, tile)
        )
        group(send.at[i, c], recv.at[i, c], disp_send.at[i, c], disp_recv.at[i, c])
        recv[i, c, p] = send[i, c, p]

    def upward(i, c):
        wait_group(recv.at[i, c], disp_recv.at[i, c])
        x = recv[i, c].reshape(per_plane * cap, tile)
        for f in range(0, ff, 256):
            a = dot(x, wg[c * tile : (c + 1) * tile, f : f + 256])
            b = dot(x, wu[c * tile : (c + 1) * tile, f : f + 256])
            if c > 0:
                a = acc_gate[:, f : f + 256] + a
                b = acc_up[:, f : f + 256] + b
            if c < PARTS - 1:
                acc_gate[:, f : f + 256] = a
                acc_up[:, f : f + 256] = b
            else:
                hidden[:, f : f + 256] = (a / (1.0 + jnp.exp(-a)) * b).astype(BF16)

    def downward(i):
        for c in range(PARTS):
            outb[i, c] = (
                dot(hidden[...], wd[:, c * tile : (c + 1) * tile])
                .astype(BF16)
                .reshape(per_plane, cap, tile)
            )
            group(outb.at[i, c], ret.at[i, c], back_send.at[i, c], back_recv.at[i, c])
            ret[i, c, p] = outb[i, c, p]

    spread_back = {}

    def part_copy(i, c, slot, device):
        return remote(
            part_out.at[i - 1, c], part_in.at[slot, c],
            part_send.at[i - 1, c], part_recv.at[slot, c], device,
        )

    def combine(i, c):
        if i not in spread_back:
            spread_back[i] = (from_slots(i), gate_columns(i))
        wait_group(ret.at[i, c], back_recv.at[i, c])
        given = ret[i, c].reshape(per_plane * cap, tile)
        part = sum(gate * dot(pick, given) for pick, gate in zip(*spread_back[i]))
        if i == 0:
            resid[c] += part
            return

        @pl.when(is_end)
        def _():
            part_out[i - 1, c] = part.astype(BF16)
            part_copy(i, c, planes if i == 1 else order[i], inward).start()

        @pl.when(is_middle)
        def _():
            local[i - 1, c] = part

    def relay(i, c):
        wait_for(part_in.at[order[i], c], part_recv.at[order[i], c])
        part_out[i - 1, c] = (local[i - 1, c] + part_in[order[i], c].astype(F32)).astype(BF16)
        part_copy(i, c, order[i], outward if i == 1 else inward).start()

    def finish(c, both):
        part = resid[c]
        if both:
            wait_for(part_in.at[planes, c], part_recv.at[planes, c])
            part = part + part_in[planes, c].astype(F32)
        wait_for(part_in.at[z, c], part_recv.at[z, c])
        out[:, c * tile : (c + 1) * tile] = (part + part_in[z, c].astype(F32)).astype(BF16)

    for c in range(PARTS):
        block[z, c] = (
            resid[c] * scale * gain[:, c * tile : (c + 1) * tile]
        ).astype(BF16)

        if c < 2:
            own_in(c).start()
        else:

            @pl.when(is_end)
            def _():
                own_in(c).start()

        @pl.when(is_middle)
        def _():
            own_out(c).start()

        dispatch(0, c)

    for i in range(1, planes):
        wait_for(meta.at[order[i]], meta_recv.at[order[i]])
    for load in loads[1:3]:
        load.wait()
    picks.append(to_slots(1))
    upward(0, 0)
    forward(1, 0)
    dispatch(1, 0)
    upward(0, 1)
    upward(0, 2)
    forward(1, 1)
    dispatch(1, 1)
    upward(0, 3)
    loads[3].wait()
    downward(0)
    forward(1, 2)
    dispatch(1, 2)
    forward(2, 0)
    picks.append(to_slots(2))
    combine(0, 0)
    upward(1, 0)
    forward(1, 3)

    @pl.when(is_middle)
    def _():
        for c in range(2, PARTS):
            own_in(c).start()

    dispatch(1, 3)
    forward(2, 1)
    combine(0, 1)
    combine(0, 2)
    upward(1, 1)
    forward(2, 2)
    combine(0, 3)
    upward(1, 2)
    dispatch(2, 0)
    upward(1, 3)
    downward(1)
    forward(2, 3)
    forward(3, 0)
    forward(3, 1)
    dispatch(2, 1)
    picks.append(to_slots(3))
    combine(1, 0)
    upward(2, 0)
    combine(1, 1)
    dispatch(2, 2)
    forward(3, 2)
    combine(1, 2)
    upward(2, 1)
    combine(1, 3)
    dispatch(2, 3)
    forward(3, 3)
    upward(2, 2)
    dispatch(3, 0)
    upward(2, 3)
    downward(2)
    dispatch(3, 1)
    combine(2, 0)
    upward(3, 0)
    combine(2, 1)
    dispatch(3, 2)
    combine(2, 2)
    upward(3, 1)
    combine(2, 3)
    dispatch(3, 3)
    upward(3, 2)
    upward(3, 3)
    downward(3)
    for c in range(PARTS):
        combine(3, c)

    @pl.when(is_end)
    def _():
        for c in range(PARTS):
            finish(c, False)

    @pl.when(is_middle)
    def _():
        for i, c in (
            (2, 0), (2, 1), (1, 0), (2, 2), (1, 1), (2, 3), (1, 2), (3, 0), (1, 3), (3, 1),
            (0, 0), (3, 2), (0, 1), (3, 3), (0, 2), (0, 3),
        ):
            if i:
                relay(i, c)
            else:
                finish(c, True)

    for copy in metas:
        copy.wait_send()
    for c in range(PARTS):
        own_in(c).wait_send()
        for i in range(planes):
            wait_group(send.at[i, c], disp_send.at[i, c])
            wait_group(outb.at[i, c], back_send.at[i, c])
        for i in range(1, planes):
            wait_for(part_out.at[i - 1, c], part_send.at[i - 1, c])

    @pl.when(is_middle)
    def _():
        for c in range(PARTS):
            own_out(c).wait_send()
            for i in range(1, planes):
                onward(i, c).wait_send()


def fused(
    tp_size, planes, per_plane, cap,
    stream, outer_gate, inner_gate, conv_values, doc_ids, conv_taps, out_weight, norm_gain,
    route_ids, route_logits, group_weight, w_gate, w_up, w_down,
):
    rows, width = stream.shape
    length, chan = inner_gate.shape
    ff = w_gate.shape[2]
    tile = width // PARTS
    vmem = pl.BlockSpec(memory_space=pltpu.VMEM)
    anywhere = pl.BlockSpec(memory_space=pl.ANY)
    slotted = pltpu.VMEM((planes, PARTS, per_plane, cap, tile), BF16)
    dma = pltpu.SemaphoreType.DMA
    return pl.pallas_call(
        functools.partial(fused_kernel, tp_size, planes, per_plane, cap),
        out_shape=jax.ShapeDtypeStruct((rows, width), BF16),
        in_specs=[vmem] * 10 + [anywhere] * 4,
        out_specs=vmem,
        scratch_shapes=[
            pltpu.VMEM(out_weight.shape, BF16),
            pltpu.VMEM((width, ff), BF16),
            pltpu.VMEM((width, ff), BF16),
            pltpu.VMEM((ff, width), BF16),
            pltpu.VMEM((2, 16, chan), BF16),
            pltpu.VMEM((2, 16, chan), BF16),
            pltpu.VMEM((2, 1, length), jnp.int32),
            pltpu.VMEM((tp_size, rows, chan), BF16),
            pltpu.VMEM((rows, chan), BF16),
            pltpu.VMEM((PARTS, rows, tile), F32),
            pltpu.VMEM((planes, 8, rows), F32),
            pltpu.VMEM((planes, PARTS, rows, tile), BF16),
            slotted, slotted, slotted, slotted,
            pltpu.VMEM((per_plane * cap, ff), F32),
            pltpu.VMEM((per_plane * cap, ff), F32),
            pltpu.VMEM((per_plane * cap, ff), BF16),
            pltpu.VMEM((planes - 1, PARTS, rows, tile), F32),
            pltpu.VMEM((planes - 1, PARTS, rows, tile), BF16),
            pltpu.VMEM((planes + 1, PARTS, rows, tile), BF16),
            dma((4,)), dma((4,)), dma((4,)), dma, dma, dma((planes - 1,)), dma((planes,)),
            dma((2, PARTS)), dma((3, PARTS)), dma((planes, PARTS)),
            dma((planes, PARTS)), dma((planes, PARTS)),
            dma((planes, PARTS)), dma((planes, PARTS)),
            dma((planes - 1, PARTS)), dma((planes + 1, PARTS)),
        ],
        compiler_params=pltpu.CompilerParams(
            collective_id=0, has_side_effects=True, vmem_limit_bytes=56 * 1024 * 1024
        ),
    )(
        stream, outer_gate, inner_gate, conv_values, doc_ids[None, :], conv_taps,
        norm_gain[None, :], route_ids.T, route_logits.T, group_weight[None, :],
        out_weight, w_gate, w_up, w_down,
    )


def body(*args):
    stream, route_ids = args[0], args[8]
    tp_size = lax.axis_size("tp")
    total = lax.axis_size("sp") * tp_size
    top = route_ids.shape[1]
    cap = 2 * stream.shape[0] * top // total
    planes = 4
    per_plane = total // planes
    if tp_size != 2 or top != 2 or total % planes or cap % 16 or per_plane * cap != stream.shape[0]:
        return on_device(*args)
    return fused(tp_size, planes, per_plane, cap, *args)


def solution(mesh):
    placed = (
        P(("sp", "tp"), None),
        P("sp", "tp"),
        P("sp", "tp"),
        P("sp", "tp"),
        P("sp"),
        P(None, "tp"),
        P(),
        P(),
        P(("sp", "tp"), None),
        P(("sp", "tp"), None),
        P(("sp", "tp")),
        P(("sp", "tp"), None, None),
        P(("sp", "tp"), None, None),
        P(("sp", "tp"), None, None),
    )
    return jax.shard_map(
        body, mesh=mesh, in_specs=placed, out_specs=P(("sp", "tp"), None), check_vma=False
    )
```

```python
import functools

import jax
import jax.numpy as jnp
from jax import lax
from jax.experimental import pallas as pl
from jax.experimental.pallas import tpu as pltpu
from jax.sharding import PartitionSpec as P


def padded_2(shard, sides, width):
    for axis, dim in sides:
        size, length = (lax.axis_size(axis), shard.shape[dim])
        up = [(i, (i + 1) % size) for i in range(size - 1)]
        down = [(j, i) for i, j in up]
        last = lax.slice_in_dim(shard, length - width, length, axis=dim)
        leading = lax.slice_in_dim(shard, 0, width, axis=dim)
        before = lax.ppermute(last, axis, up)
        after = lax.ppermute(leading, axis, down)
        shard = jnp.concatenate([before, shard, after], axis=dim)
    return shard


def on_device(
    stream,
    outer_gate,
    inner_gate,
    conv_values,
    doc_ids,
    conv_taps,
    out_weight,
    norm_gain,
    route_ids,
    route_logits,
    group_weight,
    w_gate,
    w_up,
    w_down,
):
    tok_rows = stream.shape[0]
    width = stream.shape[1]
    product = (inner_gate.astype(jnp.float32) * conv_values.astype(jnp.float32)).astype(
        jnp.bfloat16
    )
    doc_float = doc_ids.astype(jnp.bfloat16)
    padded, padded_docs = (padded_2(product, (("sp", 0),), 1), padded_2(doc_float, (("sp", 0),), 1))
    same_prev = (padded_docs[:-2] == doc_float).astype(jnp.float32)[:, None]
    same_next = (padded_docs[2:] == doc_float).astype(jnp.float32)[:, None]
    conv = (
        conv_taps[0] * padded[:-2].astype(jnp.float32) * same_prev
        + conv_taps[1] * product.astype(jnp.float32)
        + conv_taps[2] * padded[2:].astype(jnp.float32) * same_next
    )
    mixed = (outer_gate.astype(jnp.float32) * conv).astype(jnp.bfloat16)
    channels = lax.all_to_all(mixed, "tp", split_axis=0, concat_axis=1, tiled=True)
    projected = jnp.dot(channels, out_weight, preferred_element_type=jnp.float32)
    resid = stream.astype(jnp.float32) + projected
    scale = lax.rsqrt(jnp.mean(resid * resid, axis=-1, keepdims=True) + 1e-06)
    normed = (resid * scale * norm_gain).astype(jnp.bfloat16)
    expert_total = lax.axis_size("sp") * lax.axis_size("tp")
    top_count = route_ids.shape[1]
    capacity = 2 * tok_rows * top_count // expert_total
    flat_ids = route_ids.reshape(-1)
    one_hot = (flat_ids[:, None] == jnp.arange(expert_total, dtype=jnp.int32)[None, :]).astype(
        jnp.int32
    )
    rank = jnp.sum((jnp.cumsum(one_hot, axis=0) - 1) * one_hot, axis=1)
    slot = flat_ids * capacity + rank
    slot_count = expert_total * capacity
    source_row = (
        jnp.zeros((slot_count,), jnp.int32)
        .at[slot]
        .set(jnp.arange(flat_ids.shape[0], dtype=jnp.int32) // top_count)
    )
    filled = jnp.zeros((slot_count,), jnp.bool_).at[slot].set(True)
    outgoing = jnp.where(filled[:, None], normed[source_row], jnp.zeros((), jnp.bfloat16)).reshape(
        expert_total, capacity, width
    )
    arrived = lax.all_to_all(outgoing, ("sp", "tp"), split_axis=0, concat_axis=0, tiled=True)
    sources, items, features = arrived.shape
    rows_in = arrived.reshape(sources * items, features)
    hidden = (
        jax.nn.silu(jnp.dot(rows_in, w_gate[0], preferred_element_type=jnp.float32))
        * jnp.dot(rows_in, w_up[0], preferred_element_type=jnp.float32)
    ).astype(jnp.bfloat16)
    outputs = jnp.dot(hidden, w_down[0], preferred_element_type=jnp.float32).astype(jnp.bfloat16)
    returned = lax.all_to_all(
        outputs.reshape(sources, items, features),
        ("sp", "tp"),
        split_axis=0,
        concat_axis=0,
        tiled=True,
    )
    picked = (
        returned.reshape(slot_count, width)[slot]
        .astype(jnp.float32)
        .reshape(tok_rows, top_count, width)
    )
    expo = jnp.exp(route_logits)
    gate = group_weight[:, None] * expo / jnp.sum(expo, axis=1, keepdims=True)
    result = resid + jnp.sum(gate[:, :, None] * picked, axis=1)
    return result.astype(jnp.bfloat16)


MESH = pl.DeviceIdType.MESH
F32, BF16 = jnp.float32, jnp.bfloat16


def dot(a, b):
    return jnp.dot(a, b, preferred_element_type=F32)


PARTS = 4


def fused_kernel(
    tp_size, planes, per_plane, cap,
    docs, taps, gain, ids, logits, weight,
    inner_hbm, values_hbm, outer_hbm, stream_hbm, ow_hbm, wg_hbm, wu_hbm, wd_hbm,
    out,
    inner, values, outer, stream, ow, wg, wu, wd,
    product, product_in, outer_in, taps_in, edge_out, edge_in, doc_in, resid, result,
    meta, block, send, recv, outb, ret, acc_gate, acc_up, hidden, local, part_out, part_in,
    load_sem, edge_send, edge_recv, swap_send, swap_recv, meta_send, meta_recv,
    in_send, out_send, hop_recv, disp_send, disp_recv, back_send, back_recv,
    part_send, part_recv, result_sem,
):
    sp, tp = lax.axis_index("sp"), lax.axis_index("tp")
    sp_size = planes * per_plane // tp_size
    total = planes * per_plane
    me = sp * tp_size + tp
    z, p = me // per_plane, me % per_plane
    rows, width = stream.shape
    length, chan = inner.shape
    tile = width // PARTS
    top = ids.shape[0]
    ff = hidden.shape[1]
    other = 1 - tp

    middle = (z % 3 + 1) // 2
    is_middle, is_end = middle == 1, middle == 0
    step = 1 - 2 * (z // 2)
    order = [z, z + step * (1 - 2 * middle), z + step * (3 - middle), z + step * (2 - middle)]

    def place(index):
        return (index // tp_size, index % tp_size)

    inward = place((z + step) * per_plane + p)
    outward = place((z - step) * per_plane + p)

    def remote(src, dst, source_sem, target_sem, device):
        return pltpu.make_async_remote_copy(
            src_ref=src, dst_ref=dst, send_sem=source_sem, recv_sem=target_sem,
            device_id=device, device_id_type=MESH,
        )

    def wait_for(ref, sem):
        pltpu.make_async_copy(ref, ref, sem).wait()

    loads = [
        pltpu.make_async_copy(src, dst, load_sem.at[i])
        for i, (src, dst) in enumerate(
            (
                (inner_hbm, inner), (values_hbm, values), (outer_hbm, outer),
                (stream_hbm, stream), (ow_hbm, ow),
                (wg_hbm.at[0], wg), (wu_hbm.at[0], wu), (wd_hbm.at[0], wd),
            )
        )
    ]
    for load in loads:
        load.start()

    has_left, has_right = sp > 0, sp < sp_size - 1
    barrier = pltpu.get_barrier_semaphore()

    def greet(device):
        pl.semaphore_signal(barrier, inc=1, device_id=device, device_id_type=MESH)

    @pl.when((tp == 0) & has_left)
    def _():
        for q in range(tp_size):
            greet((sp - 1, q))

    @pl.when((tp == 1) & has_right)
    def _():
        for q in range(tp_size):
            greet((sp + 1, q))

    for d in range(1, planes):
        greet(place((z + d) % planes * per_plane + p))
    for d in range(1, per_plane):
        greet(place(z * per_plane + (p + d) % per_plane))

    expo = jnp.exp(logits[...])
    gates = weight[...] * expo / jnp.sum(expo, axis=0, keepdims=True)
    meta[z] = jnp.concatenate([ids[...].astype(F32), gates, ids[...].astype(F32), gates], axis=0)

    @pl.when(((tp == 0) & (sp == 0)) | ((tp == 1) & (sp == sp_size - 1)))
    def _():
        edge_in[...] = jnp.zeros_like(edge_in)
        doc_in[...] = jnp.zeros_like(doc_in)

    for load in loads[:2]:
        load.wait()
    product[...] = (inner[...].astype(F32) * values[...].astype(F32)).astype(BF16)
    edge_out[0] = product[:16]
    edge_out[1] = product[length - 16 :]
    loads[2].wait()
    pl.semaphore_wait(
        barrier,
        planes + per_plane - 2 + (sp + sp_size - 1) // sp_size + (2 * sp_size - 2 - sp) // sp_size,
    )

    def edge_copies(side, device):
        return [
            remote(
                source, target.at[tp], edge_send.at[2 * side + kind], edge_recv.at[tp, kind], device
            )
            for kind, (source, target) in enumerate(((edge_out.at[side], edge_in), (docs, doc_in)))
        ]

    to_right, to_left = edge_copies(1, (sp + 1, 0)), edge_copies(0, (sp - 1, 1))

    @pl.when(has_right)
    def _():
        for copy in to_right:
            copy.start()

    @pl.when(has_left)
    def _():
        for copy in to_left:
            copy.start()

    span = rows + 16
    swaps = [
        remote(src, dst, swap_send.at[i], swap_recv.at[i], (sp, other))
        for i, (src, dst) in enumerate(
            (
                (product.at[pl.ds(pl.multiple_of(other * (rows - 16), 16), span)], product_in),
                (outer.at[pl.ds(pl.multiple_of(other * rows, rows), rows)], outer_in),
                (taps, taps_in),
            )
        )
    ]
    for copy in swaps:
        copy.start()

    metas = []
    for d in range(1, planes):
        there = place((z + d) % planes * per_plane + p)
        metas.append(remote(meta.at[z], meta.at[z], meta_send.at[d - 1], meta_recv.at[z], there))
    for copy in metas:
        copy.start()

    before = (
        lax.broadcasted_iota(jnp.int32, (rows, rows), 0)
        < lax.broadcasted_iota(jnp.int32, (rows, rows), 1)
    ).astype(F32).astype(BF16)
    rank_of = lax.broadcasted_iota(jnp.int32, (per_plane, cap, rows), 1).astype(F32)
    expert = (
        lax.broadcasted_iota(jnp.int32, (per_plane, rows), 0) + z * per_plane
    ).astype(F32)

    def slots(i):
        table = meta[order[i]]
        hits = [(table[k : k + 1] == expert).astype(F32) for k in range(top)]
        named = sum(hits)
        ahead = dot(named.astype(BF16), before)

        def spread(hit):
            at = jnp.where(hit > 0, ahead, -1.0)
            grid = jnp.broadcast_to(at[:, None, :], (per_plane, cap, rows))
            return jnp.where(grid == rank_of, 1.0, 0.0).reshape(per_plane * cap, rows)

        return named, hits, spread

    def to_slots(i):
        named, _, spread = slots(i)
        return spread(named).astype(BF16)

    def from_slots(i):
        _, hits, spread = slots(i)
        return [jnp.transpose(spread(hit)).astype(BF16) for hit in hits]

    def gate_columns(i):
        table = meta[order[i]]
        return [
            jnp.transpose(jnp.broadcast_to(table[top + k : top + k + 1], (rows, rows)))[:, :1]
            for k in range(top)
        ]

    picks = [to_slots(0)]

    row_at = lax.broadcasted_iota(jnp.int32, (rows, chan), 0)
    prod = product[pl.ds(pl.multiple_of(tp * rows, rows), rows)].astype(F32)
    seam = [product[rows - 16 : rows].astype(F32)[15:], product[rows : rows + 16].astype(F32)[:1]]
    for copy in swaps:
        copy.wait_recv()
    prod_in = product_in[pl.ds(pl.multiple_of(tp * 16, 16), rows)].astype(F32)
    seam_in = [product_in[:16].astype(F32)[15:], product_in[rows:].astype(F32)[:1]]

    @pl.when(((tp == 0) & has_left) | ((tp == 1) & has_right))
    def _():
        for q in range(tp_size):
            wait_for(edge_in.at[q], edge_recv.at[q, 0])
            wait_for(doc_in.at[q], edge_recv.at[q, 1])

    doc = jnp.broadcast_to(docs[...], (8, length))
    beyond = jnp.broadcast_to(doc_in[0], (8, length))
    lane = lax.broadcasted_iota(jnp.int32, (8, length), 1)
    prior = pltpu.roll(jnp.where(lane == length - 1, beyond, doc), 1, axis=1)
    later = pltpu.roll(jnp.where(lane == 0, beyond, doc), length - 1, axis=1)
    spot = lane + sp * length
    same_prev = jnp.where((prior == doc) & (spot > 0), 1.0, 0.0)
    same_next = jnp.where((later == doc) & (spot < sp_size * length - 1), 1.0, 0.0)

    def column(row):
        mine = jnp.where(tp == 0, row[:1, :rows], row[:1, rows:])
        return jnp.transpose(jnp.broadcast_to(mine, (128, rows)))[:, :1]

    before_col, after_col = column(same_prev), column(same_next)

    def mix(values_f, ends, edge, weights, gate):
        first = jnp.where(tp == 0, edge[15:], ends[0])
        last = jnp.where(tp == 0, ends[1], edge[:1])
        prev = jnp.where(row_at == 0, first, pltpu.roll(values_f, 1, axis=0))
        nxt = jnp.where(row_at == rows - 1, last, pltpu.roll(values_f, rows - 1, axis=0))
        conv = (
            weights[0:1] * prev * before_col
            + weights[1:2] * values_f
            + weights[2:3] * nxt * after_col
        )
        return (gate.astype(F32) * conv).astype(BF16)

    mine = mix(
        prod, seam, edge_in[tp].astype(F32), taps[...],
        outer[pl.ds(pl.multiple_of(tp * rows, rows), rows)],
    )
    theirs = mix(prod_in, seam_in, edge_in[other].astype(F32), taps_in[...], outer_in[...])
    loads[3].wait()
    loads[4].wait()
    squares = jnp.zeros((rows, 1), F32)
    for c in range(PARTS):
        cols = slice(c * tile, (c + 1) * tile)
        part = (
            stream[:, cols].astype(F32)
            + dot(mine, ow[pl.ds(pl.multiple_of(tp * chan, chan), chan), cols])
            + dot(theirs, ow[pl.ds(pl.multiple_of(other * chan, chan), chan), cols])
        )
        resid[c] = part
        squares = squares + jnp.sum(part * part, axis=1, keepdims=True)
    scale = lax.rsqrt(squares / width + 1e-06)

    def hop(j, c, sem, device):
        return remote(block.at[j, c], block.at[j, c], sem, hop_recv.at[j, c], device)

    def own_in(c):
        return hop(z, c, in_send.at[0, c], inward)

    def own_out(c):
        return hop(z, c, out_send.at[0, c], outward)

    def onward(i, c):
        if i == 1:
            return hop(order[1], c, in_send.at[1, c], inward)
        return hop(order[i], c, out_send.at[i - 1, c], outward)

    def forward(i, c):
        wait_for(block.at[order[i], c], hop_recv.at[order[i], c])
        onward(i, c).start()

    def group(src, dst, source_sem, target_sem):
        def one(i, carry):
            peer = (p + i) % per_plane
            remote(
                src.at[peer], dst.at[p], source_sem, target_sem, place(z * per_plane + peer)
            ).start()
            return carry

        lax.fori_loop(1, per_plane, one, 0)

    def wait_group(buf, sem):
        wait_for(buf.at[pl.ds(0, per_plane - 1)], sem)

    def dispatch(i, c):
        if i > 0 and not relaying[0]:
            wait_for(block.at[order[i], c], hop_recv.at[order[i], c])
        send[i, c] = (
            dot(picks[i], block[order[i], c]).astype(BF16).reshape(per_plane, cap, tile)
        )
        group(send.at[i, c], recv.at[i, c], disp_send.at[i, c], disp_recv.at[i, c])
        recv[i, c, p] = send[i, c, p]

    def upward(i, c):
        wait_group(recv.at[i, c], disp_recv.at[i, c])
        x = recv[i, c].reshape(per_plane * cap, tile)
        for f in range(0, ff, 256):
            a = dot(x, wg[c * tile : (c + 1) * tile, f : f + 256])
            b = dot(x, wu[c * tile : (c + 1) * tile, f : f + 256])
            if c > 0:
                a = acc_gate[:, f : f + 256] + a
                b = acc_up[:, f : f + 256] + b
            if c < PARTS - 1:
                acc_gate[:, f : f + 256] = a
                acc_up[:, f : f + 256] = b
            else:
                hidden[:, f : f + 256] = (a / (1.0 + jnp.exp(-a)) * b).astype(BF16)

    def downward(i):
        for c in range(PARTS):
            outb[i, c] = (
                dot(hidden[...], wd[:, c * tile : (c + 1) * tile])
                .astype(BF16)
                .reshape(per_plane, cap, tile)
            )
            group(outb.at[i, c], ret.at[i, c], back_send.at[i, c], back_recv.at[i, c])
            ret[i, c, p] = outb[i, c, p]

    spread_back, relaying = {}, [False]

    def part_copy(i, c, slot, device):
        return remote(
            part_out.at[i - 1, c], part_in.at[slot, c],
            part_send.at[i - 1, c], part_recv.at[slot, c], device,
        )

    def combine(i, c):
        if i not in spread_back:
            spread_back[i] = (from_slots(i), gate_columns(i))
        wait_group(ret.at[i, c], back_recv.at[i, c])
        given = ret[i, c].reshape(per_plane * cap, tile)
        part = sum(gate * dot(pick, given) for pick, gate in zip(*spread_back[i]))
        if i == 0:
            resid[c] += part
            return

        if relaying[0]:
            local[i - 1, c] = part
        else:
            part_out[i - 1, c] = part.astype(BF16)
            part_copy(i, c, planes if i == 1 else order[i], inward).start()

    def relay(i, c):
        wait_for(part_in.at[order[i], c], part_recv.at[order[i], c])
        part_out[i - 1, c] = (local[i - 1, c] + part_in[order[i], c].astype(F32)).astype(BF16)
        part_copy(i, c, order[i], outward if i == 1 else inward).start()

    def deliver(c):
        return pltpu.make_async_copy(
            result.at[c], out.at[:, pl.ds(c * tile, tile)], result_sem.at[c]
        )

    def finish(c, both):
        part = resid[c]
        if both:
            wait_for(part_in.at[planes, c], part_recv.at[planes, c])
            part = part + part_in[planes, c].astype(F32)
        wait_for(part_in.at[z, c], part_recv.at[z, c])
        result[c] = (part + part_in[z, c].astype(F32)).astype(BF16)
        deliver(c).start()

    for c in range(PARTS):
        block[z, c] = (
            resid[c] * scale * gain[:, c * tile : (c + 1) * tile]
        ).astype(BF16)

        if c < 2:
            own_in(c).start()
        else:

            @pl.when(is_end)
            def _():
                own_in(c).start()

        @pl.when(is_middle)
        def _():
            own_out(c).start()

        dispatch(0, c)

    for i in range(1, planes):
        wait_for(meta.at[order[i]], meta_recv.at[order[i]])
    for load in loads[5:7]:
        load.wait()

    def own_rest():
        for c in range(2, PARTS):
            own_in(c).start()

    def run(plan, relays):
        relaying[0] = relays
        picks[1:] = []
        spread_back.clear()
        steps = {
            "U": upward, "D": dispatch, "F": forward, "C": combine, "R": relay,
            "E": lambda i, c: finish(c, i == 1),
            "N": lambda i, c: downward(i),
            "P": lambda i, c: picks.append(to_slots(i)),
            "W": lambda i, c: loads[7].wait(),
            "O": lambda i, c: own_rest(),
        }
        for name in " ".join(plan).split():
            steps[name[0]](int(name[1]), int(name[2]))

    @pl.when(is_end)
    def _():
        run(
            (
                "U00 U01 U02 P10", "D10 U03 W00 N00", "D11 D12 C00 U10", "D13 U11 C01 C02",
                "C03 U12 P20 D20", "U13 D21 N10 U20", "D22 U21 C10 D23", "C11 C12 P30 D30",
                "C13 U22 D31 U23", "N20 D32 U30 U31", "C20 D33 C21 C22", "C23 U32 U33 N30",
                "C30 C31 C32 C33", "E00 E01 E02 E03",
            ),
            False,
        )

    @pl.when(is_middle)
    def _():
        run(
            (
                "P10 U00 F10 D10", "U01 U02 F11 D11", "U03 W00 N00 F12", "D12 P20 F20 D20",
                "F13 O00 D13 F21", "D21 U10 U11 C00", "C01 F22 D22 C02", "C03 F23 D23 U12",
                "P30 U13 N10 F30", "F31 D30 D31 U20", "U21 F32 D32 U22", "U23 F33 D33 N20",
                "C10 C11 C12 C13", "U30 U31 U32 U33", "N30 C20 C21 R20", "C22 C23 R21 C30",
                "R10 C31 R22 C32", "R11 C33 R23 R12", "R30 R13 R31 R32", "E10 R33 E11 E12", "E13",
            ),
            True,
        )

    for copy in metas + swaps:
        copy.wait_send()

    @pl.when(has_right)
    def _():
        for copy in to_right:
            copy.wait_send()

    @pl.when(has_left)
    def _():
        for copy in to_left:
            copy.wait_send()

    for c in range(PARTS):
        own_in(c).wait_send()
        for i in range(planes):
            wait_group(send.at[i, c], disp_send.at[i, c])
            wait_group(outb.at[i, c], back_send.at[i, c])
        for i in range(1, planes):
            wait_for(part_out.at[i - 1, c], part_send.at[i - 1, c])

    @pl.when(is_middle)
    def _():
        for c in range(PARTS):
            own_out(c).wait_send()
            for i in range(1, planes):
                onward(i, c).wait_send()

    for c in range(PARTS):
        deliver(c).wait()


def fused(
    tp_size, planes, per_plane, cap,
    stream, outer_gate, inner_gate, conv_values, doc_ids, conv_taps, out_weight, norm_gain,
    route_ids, route_logits, group_weight, w_gate, w_up, w_down,
):
    rows, width = stream.shape
    length, chan = inner_gate.shape
    ff = w_gate.shape[2]
    tile = width // PARTS
    vmem = pl.BlockSpec(memory_space=pltpu.VMEM)
    anywhere = pl.BlockSpec(memory_space=pl.ANY)
    slotted = pltpu.VMEM((planes, PARTS, per_plane, cap, tile), BF16)
    dma = pltpu.SemaphoreType.DMA
    return pl.pallas_call(
        functools.partial(fused_kernel, tp_size, planes, per_plane, cap),
        out_shape=jax.ShapeDtypeStruct((rows, width), BF16),
        in_specs=[vmem] * 6 + [anywhere] * 8,
        out_specs=anywhere,
        scratch_shapes=[
            pltpu.VMEM((length, chan), BF16),
            pltpu.VMEM((length, chan), BF16),
            pltpu.VMEM((length, chan), BF16),
            pltpu.VMEM((rows, width), BF16),
            pltpu.VMEM(out_weight.shape, BF16),
            pltpu.VMEM((width, ff), BF16),
            pltpu.VMEM((width, ff), BF16),
            pltpu.VMEM((ff, width), BF16),
            pltpu.VMEM((length, chan), BF16),
            pltpu.VMEM((rows + 16, chan), BF16),
            pltpu.VMEM((rows, chan), BF16),
            pltpu.VMEM(conv_taps.shape, F32),
            pltpu.VMEM((2, 16, chan), BF16),
            pltpu.VMEM((2, 16, chan), BF16),
            pltpu.VMEM((2, 1, length), jnp.int32),
            pltpu.VMEM((PARTS, rows, tile), F32),
            pltpu.VMEM((PARTS, rows, tile), BF16),
            pltpu.VMEM((planes, 8, rows), F32),
            pltpu.VMEM((planes, PARTS, rows, tile), BF16),
            slotted, slotted, slotted, slotted,
            pltpu.VMEM((per_plane * cap, ff), F32),
            pltpu.VMEM((per_plane * cap, ff), F32),
            pltpu.VMEM((per_plane * cap, ff), BF16),
            pltpu.VMEM((planes - 1, PARTS, rows, tile), F32),
            pltpu.VMEM((planes - 1, PARTS, rows, tile), BF16),
            pltpu.VMEM((planes + 1, PARTS, rows, tile), BF16),
            dma((8,)), dma((4,)), dma((2, 2)), dma((3,)), dma((3,)), dma((planes - 1,)), dma((planes,)),
            dma((2, PARTS)), dma((3, PARTS)), dma((planes, PARTS)),
            dma((planes, PARTS)), dma((planes, PARTS)),
            dma((planes, PARTS)), dma((planes, PARTS)),
            dma((planes - 1, PARTS)), dma((planes + 1, PARTS)), dma((PARTS,)),
        ],
        compiler_params=pltpu.CompilerParams(
            collective_id=0, has_side_effects=True, vmem_limit_bytes=56 * 1024 * 1024
        ),
    )(
        doc_ids[None, :], conv_taps, norm_gain[None, :],
        route_ids.T, route_logits.T, group_weight[None, :],
        inner_gate, conv_values, outer_gate, stream, out_weight, w_gate, w_up, w_down,
    )


def body(*args):
    stream, route_ids = args[0], args[8]
    tp_size = lax.axis_size("tp")
    total = lax.axis_size("sp") * tp_size
    top = route_ids.shape[1]
    cap = 2 * stream.shape[0] * top // total
    planes = 4
    per_plane = total // planes
    if tp_size != 2 or top != 2 or total % planes or cap % 16 or per_plane * cap != stream.shape[0]:
        return on_device(*args)
    return fused(tp_size, planes, per_plane, cap, *args)


def solution(mesh):
    placed = (
        P(("sp", "tp"), None),
        P("sp", "tp"),
        P("sp", "tp"),
        P("sp", "tp"),
        P("sp"),
        P(None, "tp"),
        P(),
        P(),
        P(("sp", "tp"), None),
        P(("sp", "tp"), None),
        P(("sp", "tp")),
        P(("sp", "tp"), None, None),
        P(("sp", "tp"), None, None),
        P(("sp", "tp"), None, None),
    )
    return jax.shard_map(
        body, mesh=mesh, in_specs=placed, out_specs=P(("sp", "tp"), None), check_vma=False
    )
```

```python
import functools

import jax
import jax.numpy as jnp
from jax import lax
from jax.experimental import pallas as pl
from jax.experimental.pallas import tpu as pltpu
from jax.sharding import PartitionSpec as P


def padded_2(shard, sides, width):
    for axis, dim in sides:
        size, length = (lax.axis_size(axis), shard.shape[dim])
        up = [(i, (i + 1) % size) for i in range(size - 1)]
        down = [(j, i) for i, j in up]
        last = lax.slice_in_dim(shard, length - width, length, axis=dim)
        leading = lax.slice_in_dim(shard, 0, width, axis=dim)
        before = lax.ppermute(last, axis, up)
        after = lax.ppermute(leading, axis, down)
        shard = jnp.concatenate([before, shard, after], axis=dim)
    return shard


def on_device(
    stream,
    outer_gate,
    inner_gate,
    conv_values,
    doc_ids,
    conv_taps,
    out_weight,
    norm_gain,
    route_ids,
    route_logits,
    group_weight,
    w_gate,
    w_up,
    w_down,
):
    tok_rows = stream.shape[0]
    width = stream.shape[1]
    product = (inner_gate.astype(jnp.float32) * conv_values.astype(jnp.float32)).astype(
        jnp.bfloat16
    )
    doc_float = doc_ids.astype(jnp.bfloat16)
    padded, padded_docs = (padded_2(product, (("sp", 0),), 1), padded_2(doc_float, (("sp", 0),), 1))
    same_prev = (padded_docs[:-2] == doc_float).astype(jnp.float32)[:, None]
    same_next = (padded_docs[2:] == doc_float).astype(jnp.float32)[:, None]
    conv = (
        conv_taps[0] * padded[:-2].astype(jnp.float32) * same_prev
        + conv_taps[1] * product.astype(jnp.float32)
        + conv_taps[2] * padded[2:].astype(jnp.float32) * same_next
    )
    mixed = (outer_gate.astype(jnp.float32) * conv).astype(jnp.bfloat16)
    channels = lax.all_to_all(mixed, "tp", split_axis=0, concat_axis=1, tiled=True)
    projected = jnp.dot(channels, out_weight, preferred_element_type=jnp.float32)
    resid = stream.astype(jnp.float32) + projected
    scale = lax.rsqrt(jnp.mean(resid * resid, axis=-1, keepdims=True) + 1e-06)
    normed = (resid * scale * norm_gain).astype(jnp.bfloat16)
    expert_total = lax.axis_size("sp") * lax.axis_size("tp")
    top_count = route_ids.shape[1]
    capacity = 2 * tok_rows * top_count // expert_total
    flat_ids = route_ids.reshape(-1)
    one_hot = (flat_ids[:, None] == jnp.arange(expert_total, dtype=jnp.int32)[None, :]).astype(
        jnp.int32
    )
    rank = jnp.sum((jnp.cumsum(one_hot, axis=0) - 1) * one_hot, axis=1)
    slot = flat_ids * capacity + rank
    slot_count = expert_total * capacity
    source_row = (
        jnp.zeros((slot_count,), jnp.int32)
        .at[slot]
        .set(jnp.arange(flat_ids.shape[0], dtype=jnp.int32) // top_count)
    )
    filled = jnp.zeros((slot_count,), jnp.bool_).at[slot].set(True)
    outgoing = jnp.where(filled[:, None], normed[source_row], jnp.zeros((), jnp.bfloat16)).reshape(
        expert_total, capacity, width
    )
    arrived = lax.all_to_all(outgoing, ("sp", "tp"), split_axis=0, concat_axis=0, tiled=True)
    sources, items, features = arrived.shape
    rows_in = arrived.reshape(sources * items, features)
    hidden = (
        jax.nn.silu(jnp.dot(rows_in, w_gate[0], preferred_element_type=jnp.float32))
        * jnp.dot(rows_in, w_up[0], preferred_element_type=jnp.float32)
    ).astype(jnp.bfloat16)
    outputs = jnp.dot(hidden, w_down[0], preferred_element_type=jnp.float32).astype(jnp.bfloat16)
    returned = lax.all_to_all(
        outputs.reshape(sources, items, features),
        ("sp", "tp"),
        split_axis=0,
        concat_axis=0,
        tiled=True,
    )
    picked = (
        returned.reshape(slot_count, width)[slot]
        .astype(jnp.float32)
        .reshape(tok_rows, top_count, width)
    )
    expo = jnp.exp(route_logits)
    gate = group_weight[:, None] * expo / jnp.sum(expo, axis=1, keepdims=True)
    result = resid + jnp.sum(gate[:, :, None] * picked, axis=1)
    return result.astype(jnp.bfloat16)


MESH = pl.DeviceIdType.MESH
F32, BF16 = jnp.float32, jnp.bfloat16


def dot(a, b):
    return jnp.dot(a, b, preferred_element_type=F32)


PARTS = 4


def fused_kernel(
    tp_size, planes, per_plane, cap,
    docs, taps, gain, ids, logits, weight,
    inner_hbm, values_hbm, outer_hbm, stream_hbm, ow_hbm, wg_hbm, wu_hbm, wd_hbm,
    out,
    inner, values, outer, stream, ow, wg, wu, wd,
    product, product_in, outer_in, taps_in, edge_out, edge_in, doc_in, resid, result,
    meta, block, send, recv, outb, ret, acc_gate, acc_up, hidden, local, part_out, part_in,
    load_sem, edge_send, edge_recv, swap_send, swap_recv, meta_send, meta_recv,
    in_send, out_send, hop_recv, disp_send, disp_recv, back_send, back_recv,
    part_send, part_recv, result_sem,
):
    sp, tp = lax.axis_index("sp"), lax.axis_index("tp")
    sp_size = planes * per_plane // tp_size
    total = planes * per_plane
    me = sp * tp_size + tp
    z, p = me // per_plane, me % per_plane
    rows, width = stream.shape
    length, chan = inner.shape
    tile = width // PARTS
    top = ids.shape[0]
    ff = hidden.shape[1]
    other = 1 - tp

    middle = (z % 3 + 1) // 2
    is_middle, is_end = middle == 1, middle == 0
    step = 1 - 2 * (z // 2)
    order = [z, z + step * (1 - 2 * middle), z + step * (3 - middle), z + step * (2 - middle)]

    def place(index):
        return (index // tp_size, index % tp_size)

    inward = place((z + step) * per_plane + p)
    outward = place((z - step) * per_plane + p)

    def remote(src, dst, source_sem, target_sem, device):
        return pltpu.make_async_remote_copy(
            src_ref=src, dst_ref=dst, send_sem=source_sem, recv_sem=target_sem,
            device_id=device, device_id_type=MESH,
        )

    def wait_for(ref, sem):
        pltpu.make_async_copy(ref, ref, sem).wait()

    loads = [
        pltpu.make_async_copy(src, dst, load_sem.at[i])
        for i, (src, dst) in enumerate(
            (
                (inner_hbm, inner), (values_hbm, values), (outer_hbm, outer),
                (stream_hbm, stream), (ow_hbm, ow),
                (wg_hbm.at[0], wg), (wu_hbm.at[0], wu), (wd_hbm.at[0], wd),
            )
        )
    ]
    for load in loads:
        load.start()

    has_left, has_right = sp > 0, sp < sp_size - 1
    barrier = pltpu.get_barrier_semaphore()

    def greet(device):
        pl.semaphore_signal(barrier, inc=1, device_id=device, device_id_type=MESH)

    @pl.when((tp == 0) & has_left)
    def _():
        for q in range(tp_size):
            greet((sp - 1, q))

    @pl.when((tp == 1) & has_right)
    def _():
        for q in range(tp_size):
            greet((sp + 1, q))

    for d in range(1, planes):
        greet(place((z + d) % planes * per_plane + p))
    for d in range(1, per_plane):
        greet(place(z * per_plane + (p + d) % per_plane))

    expo = jnp.exp(logits[...])
    gates = weight[...] * expo / jnp.sum(expo, axis=0, keepdims=True)
    meta[z] = jnp.concatenate([ids[...].astype(F32), gates, ids[...].astype(F32), gates], axis=0)

    @pl.when(((tp == 0) & (sp == 0)) | ((tp == 1) & (sp == sp_size - 1)))
    def _():
        edge_in[...] = jnp.zeros_like(edge_in)
        doc_in[...] = jnp.zeros_like(doc_in)

    for load in loads[:2]:
        load.wait()
    product[...] = (inner[...].astype(F32) * values[...].astype(F32)).astype(BF16)
    edge_out[0] = product[:16]
    edge_out[1] = product[length - 16 :]
    loads[2].wait()
    pl.semaphore_wait(
        barrier,
        planes + per_plane - 2 + (sp + sp_size - 1) // sp_size + (2 * sp_size - 2 - sp) // sp_size,
    )

    def edge_copies(side, device):
        return [
            remote(
                source, target.at[tp], edge_send.at[2 * side + kind], edge_recv.at[tp, kind], device
            )
            for kind, (source, target) in enumerate(((edge_out.at[side], edge_in), (docs, doc_in)))
        ]

    to_right, to_left = edge_copies(1, (sp + 1, 0)), edge_copies(0, (sp - 1, 1))

    @pl.when(has_right)
    def _():
        for copy in to_right:
            copy.start()

    @pl.when(has_left)
    def _():
        for copy in to_left:
            copy.start()

    span = rows + 16
    swaps = [
        remote(src, dst, swap_send.at[i], swap_recv.at[i], (sp, other))
        for i, (src, dst) in enumerate(
            (
                (product.at[pl.ds(pl.multiple_of(other * (rows - 16), 16), span)], product_in),
                (outer.at[pl.ds(pl.multiple_of(other * rows, rows), rows)], outer_in),
                (taps, taps_in),
            )
        )
    ]
    for copy in swaps:
        copy.start()

    metas = []
    for d in range(1, planes):
        there = place((z + d) % planes * per_plane + p)
        metas.append(remote(meta.at[z], meta.at[z], meta_send.at[d - 1], meta_recv.at[z], there))
    for copy in metas:
        copy.start()

    before = (
        lax.broadcasted_iota(jnp.int32, (rows, rows), 0)
        < lax.broadcasted_iota(jnp.int32, (rows, rows), 1)
    ).astype(F32).astype(BF16)
    rank_of = lax.broadcasted_iota(jnp.int32, (per_plane, cap, rows), 1).astype(F32)
    expert = (
        lax.broadcasted_iota(jnp.int32, (per_plane, rows), 0) + z * per_plane
    ).astype(F32)

    def slots(i):
        table = meta[order[i]]
        hits = [(table[k : k + 1] == expert).astype(F32) for k in range(top)]
        named = sum(hits)
        ahead = dot(named.astype(BF16), before)

        def spread(hit):
            at = jnp.where(hit > 0, ahead, -1.0)
            grid = jnp.broadcast_to(at[:, None, :], (per_plane, cap, rows))
            return jnp.where(grid == rank_of, 1.0, 0.0).reshape(per_plane * cap, rows)

        return named, hits, spread

    def to_slots(i):
        named, _, spread = slots(i)
        return spread(named).astype(BF16)

    def from_slots(i):
        _, hits, spread = slots(i)
        return [jnp.transpose(spread(hit)).astype(BF16) for hit in hits]

    def gate_columns(i):
        table = meta[order[i]]
        return [
            jnp.transpose(jnp.broadcast_to(table[top + k : top + k + 1], (rows, rows)))[:, :1]
            for k in range(top)
        ]

    picks = [to_slots(0)]

    row_at = lax.broadcasted_iota(jnp.int32, (rows, chan), 0)
    prod = product[pl.ds(pl.multiple_of(tp * rows, rows), rows)].astype(F32)
    seam = [product[rows - 16 : rows].astype(F32)[15:], product[rows : rows + 16].astype(F32)[:1]]
    for copy in swaps:
        copy.wait_recv()
    prod_in = product_in[pl.ds(pl.multiple_of(tp * 16, 16), rows)].astype(F32)
    seam_in = [product_in[:16].astype(F32)[15:], product_in[rows:].astype(F32)[:1]]

    doc = jnp.broadcast_to(docs[...], (8, length))
    lane = lax.broadcasted_iota(jnp.int32, (8, length), 1)
    same_prev = jnp.where((pltpu.roll(doc, 1, axis=1) == doc) & (lane > 0), 1.0, 0.0)
    same_next = jnp.where(
        (pltpu.roll(doc, length - 1, axis=1) == doc) & (lane < length - 1), 1.0, 0.0
    )

    def column(row):
        mine = jnp.where(tp == 0, row[:1, :rows], row[:1, rows:])
        return jnp.transpose(jnp.broadcast_to(mine, (128, rows)))[:, :1]

    before_col, after_col = column(same_prev), column(same_next)

    def convolve(values_f, ends, weights):
        prev = jnp.where(row_at == 0, ends[0], pltpu.roll(values_f, 1, axis=0))
        nxt = jnp.where(row_at == rows - 1, ends[1], pltpu.roll(values_f, rows - 1, axis=0))
        return (
            weights[0:1] * prev * before_col
            + weights[1:2] * values_f
            + weights[2:3] * nxt * after_col
        )

    halves = [
        (
            convolve(prod, seam, taps[...]), taps,
            outer[pl.ds(pl.multiple_of(tp * rows, rows), rows)].astype(F32), tp,
        ),
        (convolve(prod_in, seam_in, taps_in[...]), taps_in, outer_in[...].astype(F32), other),
    ]
    mixed = [(gate * conv).astype(BF16) for conv, _, gate, _ in halves]
    loads[3].wait()
    loads[4].wait()

    def project(pieces, c):
        return sum(
            dot(piece, ow[pl.ds(pl.multiple_of(half[3] * chan, chan), chan), c * tile : (c + 1) * tile])
            for piece, half in zip(pieces, halves)
        )

    squares = jnp.zeros((rows, 1), F32)
    for c in range(PARTS):
        part = stream[:, c * tile : (c + 1) * tile].astype(F32) + project(mixed, c)
        resid[c] = part
        squares = squares + jnp.sum(part * part, axis=1, keepdims=True)
    scale = lax.rsqrt(squares / width + 1e-06)

    def first_rows(x):
        return jnp.where(tp == 0, x[:16], x[rows - 16 :])

    late = pl.ds(pl.multiple_of(tp * (rows - 16), 16), 16)
    early = pl.ds(pl.multiple_of(other * 16, 16), rows - 16)

    def hop(j, c, sem, device):
        return remote(block.at[j, c], block.at[j, c], sem, hop_recv.at[j, c], device)

    def own(c, which, sem, device):
        ref = block.at[z, c, which]
        return remote(ref, ref, sem, hop_recv.at[z, c], device)

    def own_start(c, which):
        @pl.when(is_middle)
        def _():
            own(c, which, out_send, outward).start()

        if c < 2:
            own(c, which, in_send, inward).start()
        else:

            @pl.when(is_end)
            def _():
                own(c, which, in_send, inward).start()

    def onward(i, c):
        if i == 1:
            return hop(order[1], c, in_send, inward)
        return hop(order[i], c, out_send, outward)

    def forward(i, c):
        wait_for(block.at[order[i], c], hop_recv.at[order[i], c])
        onward(i, c).start()

    def group(src, dst, source_sem, target_sem):
        def one(i, carry):
            peer = (p + i) % per_plane
            remote(
                src.at[peer], dst.at[p], source_sem, target_sem, place(z * per_plane + peer)
            ).start()
            return carry

        lax.fori_loop(1, per_plane, one, 0)

    def wait_group(buf, sem):
        wait_for(buf.at[pl.ds(0, per_plane - 1)], sem)

    def dispatch(i, c):
        if i > 0 and not relaying[0]:
            wait_for(block.at[order[i], c], hop_recv.at[order[i], c])
        send[i, c] = (
            dot(picks[i], block[order[i], c]).astype(BF16).reshape(per_plane, cap, tile)
        )
        group(send.at[i, c], recv.at[i, c], disp_send, disp_recv.at[i, c])
        recv[i, c, p] = send[i, c, p]

    def upward(i, c):
        wait_group(recv.at[i, c], disp_recv.at[i, c])
        x = recv[i, c].reshape(per_plane * cap, tile)
        for f in range(0, ff, 256):
            a = dot(x, wg[c * tile : (c + 1) * tile, f : f + 256])
            b = dot(x, wu[c * tile : (c + 1) * tile, f : f + 256])
            if c > 0:
                a = acc_gate[:, f : f + 256] + a
                b = acc_up[:, f : f + 256] + b
            if c < PARTS - 1:
                acc_gate[:, f : f + 256] = a
                acc_up[:, f : f + 256] = b
            else:
                hidden[:, f : f + 256] = (a / (1.0 + jnp.exp(-a)) * b).astype(BF16)

    def hand_back(i, c):
        group(outb.at[i, c], ret.at[i, c], back_send, back_recv.at[i, c])

    def downward(i, c, sends):
        outb[i, c] = (
            dot(hidden[...], wd[:, c * tile : (c + 1) * tile])
            .astype(BF16)
            .reshape(per_plane, cap, tile)
        )
        if sends:
            hand_back(i, c)
        ret[i, c, p] = outb[i, c, p]

    spread_back, relaying = {}, [False]

    def part_copy(i, c, slot, device):
        return remote(
            part_out.at[i - 1, c], part_in.at[slot, c],
            part_send, part_recv.at[slot, c], device,
        )

    def combine(i, c):
        if i not in spread_back:
            spread_back[i] = (from_slots(i), gate_columns(i))
        wait_group(ret.at[i, c], back_recv.at[i, c])
        given = ret[i, c].reshape(per_plane * cap, tile)
        part = sum(gate * dot(pick, given) for pick, gate in zip(*spread_back[i]))
        if i == 0:
            resid[c] += part
            return

        if relaying[0]:
            local[i - 1, c] = part
        else:
            part_out[i - 1, c] = part.astype(BF16)
            part_copy(i, c, planes if i == 1 else order[i], inward).start()

    def relay(i, c):
        wait_for(part_in.at[order[i], c], part_recv.at[order[i], c])
        part_out[i - 1, c] = (local[i - 1, c] + part_in[order[i], c].astype(F32)).astype(BF16)
        part_copy(i, c, order[i], outward if i == 1 else inward).start()

    def deliver(c):
        return pltpu.make_async_copy(
            result.at[c], out.at[:, pl.ds(c * tile, tile)], result_sem.at[c]
        )

    def finish(c, both):
        part = resid[c]
        if both:
            wait_for(part_in.at[planes, c], part_recv.at[planes, c])
            part = part + part_in[planes, c].astype(F32)
        wait_for(part_in.at[z, c], part_recv.at[z, c])
        result[c] = (part + part_in[z, c].astype(F32)).astype(BF16)
        deliver(c).start()

    def normed(part, by, c):
        return (part * by * gain[:, c * tile : (c + 1) * tile]).astype(BF16)

    for c in range(PARTS):
        block[z, c] = normed(resid[c], scale, c)
        if c < 2:
            own_start(c, early)

    @pl.when(((tp == 0) & has_left) | ((tp == 1) & has_right))
    def _():
        for q in range(tp_size):
            wait_for(edge_in.at[q], edge_recv.at[q, 0])
            wait_for(doc_in.at[q], edge_recv.at[q, 1])

    ours = jnp.where(tp == 0, docs[:, :1], docs[:, length - 1 :])
    beyond = jnp.where(tp == 0, doc_in[0][:, length - 1 :], doc_in[0][:, :1])
    inside = jnp.where(tp == 0, sp > 0, sp < sp_size - 1)
    joined = jnp.where((ours == beyond) & inside, 1.0, 0.0)
    at_edge = lax.broadcasted_iota(jnp.int32, (16, chan), 0) == tp * 15
    fixed = []
    for conv, weights, gate, half in halves:
        edge = edge_in[half].astype(F32)
        term = (
            jnp.where(tp == 0, weights[0:1], weights[2:3])
            * jnp.where(tp == 0, edge[15:], edge[:1])
            * joined
        )
        fixed.append(
            (first_rows(gate) * (first_rows(conv) + jnp.where(at_edge, term, 0.0))).astype(BF16)
        )
    squares = jnp.zeros((16, 1), F32)
    parts = []
    for c in range(PARTS):
        part = stream[late, c * tile : (c + 1) * tile].astype(F32) + project(fixed, c)
        resid[c, late] = part
        parts.append(part)
        squares = squares + jnp.sum(part * part, axis=1, keepdims=True)
    late_scale = lax.rsqrt(squares / width + 1e-06)
    for c in range(PARTS):
        block[z, c, late] = normed(parts[c], late_scale, c)
        own_start(c, late if c < 2 else pl.ds(0, rows))
    for c in range(PARTS):
        dispatch(0, c)

    for i in range(1, planes):
        wait_for(meta.at[order[i]], meta_recv.at[order[i]])
    for load in loads[5:7]:
        load.wait()

    def own_rest():
        for c in range(2, PARTS):
            hop(z, c, in_send, inward).start()

    def run(plan, relays):
        relaying[0] = relays
        picks[1:] = []
        spread_back.clear()
        steps = {
            "U": upward, "D": dispatch, "F": forward, "C": combine, "R": relay,
            "E": lambda i, c: finish(c, i == 1),
            "N": lambda i, c: downward(i, c, True),
            "K": lambda i, c: downward(i, c, False),
            "S": hand_back,
            "P": lambda i, c: picks.append(to_slots(i)),
            "W": lambda i, c: loads[7].wait(),
            "O": lambda i, c: own_rest(),
        }
        for name in " ".join(plan).split():
            steps[name[0]](int(name[1]), int(name[2]))

    @pl.when(is_end)
    def _():
        run(
            (
                "U00 P10 D10 D11", "U01 D12 U02 U03", "W00 K00 K01 K02", "K03 D13 S00 U10",
                "U11 U12 U13 N10", "N11 N12 P20 D20", "N13 C10 P30 D21", "C11 C12 U20 D22",
                "C13 U21 D23 U22", "D30 D31 U23 N20", "D32 N21 U30 D33", "N22 C20 N23 C21",
                "U31 U32 C22 U33", "N30 N31 N32 N33", "S01 S02 S03 C23", "C30 C31 C32 C33",
                "C00 C01 C02 C03", "E00 E01 E02 E03",
            ),
            False,
        )

    @pl.when(is_middle)
    def _():
        run(
            (
                "P10 U00 F10 D10", "F11 D11 U01 U02", "F12 D12 F30 P20", "U03 W00 K00 K01",
                "K02 K03 F13 O00", "D13 F20 D20 U10", "U11 F21 D21 U12", "U13 F22 D22 N10",
                "N11 N12 N13 F23", "D23 F31 P30 D30", "D31 U20 U21 F32", "D32 C10 C11 U22",
                "F33 D33 C12 C13", "U23 N20 N21 N22", "N23 U30 U31 U32", "U33 N30 N31 N32",
                "N33 S00 S01 S02", "S03 C20 R20 C21", "R21 C22 C23 R22", "C30 R10 C31 R23",
                "C32 R11 C33 R12", "C00 R30 R13 C01", "R31 C02 R32 C03", "E10 R33 E11 E12", "E13",
            ),
            True,
        )

    for copy in metas + swaps:
        copy.wait_send()

    @pl.when(has_right)
    def _():
        for copy in to_right:
            copy.wait_send()

    @pl.when(has_left)
    def _():
        for copy in to_left:
            copy.wait_send()

    most = pl.ds(0, per_plane - 1)
    wait_for(send.at[:, :, most], disp_send)
    wait_for(outb.at[:, :, most], back_send)
    wait_for(part_out, part_send)

    @pl.when(is_end)
    def _():
        wait_for(block.at[0], in_send)

    @pl.when(is_middle)
    def _():
        wait_for(block.at[pl.ds(0, 2)], in_send)
        wait_for(block.at[pl.ds(0, 3)], out_send)

    for c in range(PARTS):
        deliver(c).wait()


def fused(
    tp_size, planes, per_plane, cap,
    stream, outer_gate, inner_gate, conv_values, doc_ids, conv_taps, out_weight, norm_gain,
    route_ids, route_logits, group_weight, w_gate, w_up, w_down,
):
    rows, width = stream.shape
    length, chan = inner_gate.shape
    ff = w_gate.shape[2]
    tile = width // PARTS
    vmem = pl.BlockSpec(memory_space=pltpu.VMEM)
    anywhere = pl.BlockSpec(memory_space=pl.ANY)
    slotted = pltpu.VMEM((planes, PARTS, per_plane, cap, tile), BF16)
    dma = pltpu.SemaphoreType.DMA
    return pl.pallas_call(
        functools.partial(fused_kernel, tp_size, planes, per_plane, cap),
        out_shape=jax.ShapeDtypeStruct((rows, width), BF16),
        in_specs=[vmem] * 6 + [anywhere] * 8,
        out_specs=anywhere,
        scratch_shapes=[
            pltpu.VMEM((length, chan), BF16),
            pltpu.VMEM((length, chan), BF16),
            pltpu.VMEM((length, chan), BF16),
            pltpu.VMEM((rows, width), BF16),
            pltpu.VMEM(out_weight.shape, BF16),
            pltpu.VMEM((width, ff), BF16),
            pltpu.VMEM((width, ff), BF16),
            pltpu.VMEM((ff, width), BF16),
            pltpu.VMEM((length, chan), BF16),
            pltpu.VMEM((rows + 16, chan), BF16),
            pltpu.VMEM((rows, chan), BF16),
            pltpu.VMEM(conv_taps.shape, F32),
            pltpu.VMEM((2, 16, chan), BF16),
            pltpu.VMEM((2, 16, chan), BF16),
            pltpu.VMEM((2, 1, length), jnp.int32),
            pltpu.VMEM((PARTS, rows, tile), F32),
            pltpu.VMEM((PARTS, rows, tile), BF16),
            pltpu.VMEM((planes, 8, rows), F32),
            pltpu.VMEM((planes, PARTS, rows, tile), BF16),
            slotted, slotted, slotted, slotted,
            pltpu.VMEM((per_plane * cap, ff), F32),
            pltpu.VMEM((per_plane * cap, ff), F32),
            pltpu.VMEM((per_plane * cap, ff), BF16),
            pltpu.VMEM((planes - 1, PARTS, rows, tile), F32),
            pltpu.VMEM((planes - 1, PARTS, rows, tile), BF16),
            pltpu.VMEM((planes + 1, PARTS, rows, tile), BF16),
            dma((8,)), dma((4,)), dma((2, 2)), dma((3,)), dma((3,)), dma((planes - 1,)), dma((planes,)),
            dma, dma, dma((planes, PARTS)), dma, dma((planes, PARTS)), dma, dma((planes, PARTS)),
            dma, dma((planes + 1, PARTS)), dma((PARTS,)),
        ],
        compiler_params=pltpu.CompilerParams(
            collective_id=0, has_side_effects=True, vmem_limit_bytes=56 * 1024 * 1024
        ),
    )(
        doc_ids[None, :], conv_taps, norm_gain[None, :],
        route_ids.T, route_logits.T, group_weight[None, :],
        inner_gate, conv_values, outer_gate, stream, out_weight, w_gate, w_up, w_down,
    )


def body(*args):
    stream, route_ids = args[0], args[8]
    tp_size = lax.axis_size("tp")
    total = lax.axis_size("sp") * tp_size
    top = route_ids.shape[1]
    cap = 2 * stream.shape[0] * top // total
    planes = 4
    per_plane = total // planes
    if tp_size != 2 or top != 2 or total % planes or cap % 16 or per_plane * cap != stream.shape[0]:
        return on_device(*args)
    return fused(tp_size, planes, per_plane, cap, *args)


def solution(mesh):
    placed = (
        P(("sp", "tp"), None),
        P("sp", "tp"),
        P("sp", "tp"),
        P("sp", "tp"),
        P("sp"),
        P(None, "tp"),
        P(),
        P(),
        P(("sp", "tp"), None),
        P(("sp", "tp"), None),
        P(("sp", "tp")),
        P(("sp", "tp"), None, None),
        P(("sp", "tp"), None, None),
        P(("sp", "tp"), None, None),
    )
    return jax.shard_map(
        body, mesh=mesh, in_specs=placed, out_specs=P(("sp", "tp"), None), check_vma=False
    )
```

```python
import functools

import jax
import jax.numpy as jnp
from jax import lax
from jax.experimental import pallas as pl
from jax.experimental.pallas import tpu as pltpu
from jax.sharding import PartitionSpec as P


def padded_2(shard, sides, width):
    for axis, dim in sides:
        size, length = (lax.axis_size(axis), shard.shape[dim])
        up = [(i, (i + 1) % size) for i in range(size - 1)]
        down = [(j, i) for i, j in up]
        last = lax.slice_in_dim(shard, length - width, length, axis=dim)
        leading = lax.slice_in_dim(shard, 0, width, axis=dim)
        before = lax.ppermute(last, axis, up)
        after = lax.ppermute(leading, axis, down)
        shard = jnp.concatenate([before, shard, after], axis=dim)
    return shard


def on_device(
    stream,
    outer_gate,
    inner_gate,
    conv_values,
    doc_ids,
    conv_taps,
    out_weight,
    norm_gain,
    route_ids,
    route_logits,
    group_weight,
    w_gate,
    w_up,
    w_down,
):
    tok_rows = stream.shape[0]
    width = stream.shape[1]
    product = (inner_gate.astype(jnp.float32) * conv_values.astype(jnp.float32)).astype(
        jnp.bfloat16
    )
    doc_float = doc_ids.astype(jnp.bfloat16)
    padded, padded_docs = (padded_2(product, (("sp", 0),), 1), padded_2(doc_float, (("sp", 0),), 1))
    same_prev = (padded_docs[:-2] == doc_float).astype(jnp.float32)[:, None]
    same_next = (padded_docs[2:] == doc_float).astype(jnp.float32)[:, None]
    conv = (
        conv_taps[0] * padded[:-2].astype(jnp.float32) * same_prev
        + conv_taps[1] * product.astype(jnp.float32)
        + conv_taps[2] * padded[2:].astype(jnp.float32) * same_next
    )
    mixed = (outer_gate.astype(jnp.float32) * conv).astype(jnp.bfloat16)
    channels = lax.all_to_all(mixed, "tp", split_axis=0, concat_axis=1, tiled=True)
    projected = jnp.dot(channels, out_weight, preferred_element_type=jnp.float32)
    resid = stream.astype(jnp.float32) + projected
    scale = lax.rsqrt(jnp.mean(resid * resid, axis=-1, keepdims=True) + 1e-06)
    normed = (resid * scale * norm_gain).astype(jnp.bfloat16)
    expert_total = lax.axis_size("sp") * lax.axis_size("tp")
    top_count = route_ids.shape[1]
    capacity = 2 * tok_rows * top_count // expert_total
    flat_ids = route_ids.reshape(-1)
    one_hot = (flat_ids[:, None] == jnp.arange(expert_total, dtype=jnp.int32)[None, :]).astype(
        jnp.int32
    )
    rank = jnp.sum((jnp.cumsum(one_hot, axis=0) - 1) * one_hot, axis=1)
    slot = flat_ids * capacity + rank
    slot_count = expert_total * capacity
    source_row = (
        jnp.zeros((slot_count,), jnp.int32)
        .at[slot]
        .set(jnp.arange(flat_ids.shape[0], dtype=jnp.int32) // top_count)
    )
    filled = jnp.zeros((slot_count,), jnp.bool_).at[slot].set(True)
    outgoing = jnp.where(filled[:, None], normed[source_row], jnp.zeros((), jnp.bfloat16)).reshape(
        expert_total, capacity, width
    )
    arrived = lax.all_to_all(outgoing, ("sp", "tp"), split_axis=0, concat_axis=0, tiled=True)
    sources, items, features = arrived.shape
    rows_in = arrived.reshape(sources * items, features)
    hidden = (
        jax.nn.silu(jnp.dot(rows_in, w_gate[0], preferred_element_type=jnp.float32))
        * jnp.dot(rows_in, w_up[0], preferred_element_type=jnp.float32)
    ).astype(jnp.bfloat16)
    outputs = jnp.dot(hidden, w_down[0], preferred_element_type=jnp.float32).astype(jnp.bfloat16)
    returned = lax.all_to_all(
        outputs.reshape(sources, items, features),
        ("sp", "tp"),
        split_axis=0,
        concat_axis=0,
        tiled=True,
    )
    picked = (
        returned.reshape(slot_count, width)[slot]
        .astype(jnp.float32)
        .reshape(tok_rows, top_count, width)
    )
    expo = jnp.exp(route_logits)
    gate = group_weight[:, None] * expo / jnp.sum(expo, axis=1, keepdims=True)
    result = resid + jnp.sum(gate[:, :, None] * picked, axis=1)
    return result.astype(jnp.bfloat16)


MESH = pl.DeviceIdType.MESH
F32, BF16 = jnp.float32, jnp.bfloat16


def dot(a, b):
    return jnp.dot(a, b, preferred_element_type=F32)


PARTS = 4


def fused_kernel(
    tp_size, planes, per_plane, cap,
    inner_hbm, values_hbm, ids_hbm, logits_hbm, weight_hbm, docs_hbm, taps_hbm, outer_hbm,
    gain_hbm, stream_hbm, ow_hbm, wg_hbm, wu_hbm, wd_hbm,
    out,
    inner, values, ids, logits, weight, docs, taps, outer, gain, stream, ow, wg, wu, wd,
    product, product_in, outer_in, taps_in, edge_out, edge_in, doc_in, resid,
    meta, block, send, recv, outb, ret, acc_gate, acc_up, hidden, local, part_out, part_in,
    load_sem, edge_send, edge_recv, swap_send, swap_recv, meta_send, meta_recv,
    in_send, out_send, hop_recv, disp_send, disp_recv, back_send, back_recv,
    part_send, part_recv,
):
    sp, tp = lax.axis_index("sp"), lax.axis_index("tp")
    sp_size = planes * per_plane // tp_size
    total = planes * per_plane
    me = sp * tp_size + tp
    z, p = me // per_plane, me % per_plane
    rows, width = stream.shape
    length, chan = inner.shape
    tile = width // PARTS
    top = ids.shape[0]
    ff = hidden.shape[1]
    other = 1 - tp

    middle = (z % 3 + 1) // 2
    is_middle, is_end = middle == 1, middle == 0
    step = 1 - 2 * (z // 2)
    order = [z, z + step * (1 - 2 * middle), z + step * (3 - middle), z + step * (2 - middle)]

    def place(index):
        return (index // tp_size, index % tp_size)

    inward = place((z + step) * per_plane + p)
    outward = place((z - step) * per_plane + p)

    def remote(src, dst, source_sem, target_sem, device):
        return pltpu.make_async_remote_copy(
            src_ref=src, dst_ref=dst, send_sem=source_sem, recv_sem=target_sem,
            device_id=device, device_id_type=MESH,
        )

    def wait_for(ref, sem):
        pltpu.make_async_copy(ref, ref, sem).wait()

    loads = [
        pltpu.make_async_copy(src, dst, load_sem.at[i])
        for i, (src, dst) in enumerate(
            (
                (inner_hbm, inner), (values_hbm, values), (ids_hbm, ids), (logits_hbm, logits),
                (weight_hbm, weight), (docs_hbm, docs), (taps_hbm, taps), (outer_hbm, outer),
                (gain_hbm, gain), (stream_hbm, stream), (ow_hbm, ow),
                (wg_hbm.at[0], wg), (wu_hbm.at[0], wu), (wd_hbm.at[0], wd),
            )
        )
    ]
    for load in loads:
        load.start()

    has_left, has_right = sp > 0, sp < sp_size - 1
    barrier = pltpu.get_barrier_semaphore()

    def greet(device):
        pl.semaphore_signal(barrier, inc=1, device_id=device, device_id_type=MESH)

    @pl.when((tp == 0) & has_left)
    def _():
        for q in range(tp_size):
            greet((sp - 1, q))

    @pl.when((tp == 1) & has_right)
    def _():
        for q in range(tp_size):
            greet((sp + 1, q))

    for d in range(1, planes):
        greet(place((z + d) % planes * per_plane + p))
    for d in range(1, per_plane):
        greet(place(z * per_plane + (p + d) % per_plane))

    @pl.when(((tp == 0) & (sp == 0)) | ((tp == 1) & (sp == sp_size - 1)))
    def _():
        edge_in[...] = jnp.zeros_like(edge_in)
        doc_in[...] = jnp.zeros_like(doc_in)

    for load in loads[:2]:
        load.wait()
    product[...] = (inner[...].astype(F32) * values[...].astype(F32)).astype(BF16)
    edge_out[0] = product[:16]
    edge_out[1] = product[length - 16 :]
    for load in loads[2:8]:
        load.wait()
    expo = jnp.exp(logits[...])
    gates = weight[...] * expo / jnp.sum(expo, axis=0, keepdims=True)
    meta[z] = jnp.concatenate([ids[...].astype(F32), gates, ids[...].astype(F32), gates], axis=0)
    pl.semaphore_wait(
        barrier,
        planes + per_plane - 2 + (sp + sp_size - 1) // sp_size + (2 * sp_size - 2 - sp) // sp_size,
    )

    def edge_copies(side, device):
        return [
            remote(
                source, target.at[tp], edge_send.at[2 * side + kind], edge_recv.at[tp, kind], device
            )
            for kind, (source, target) in enumerate(((edge_out.at[side], edge_in), (docs, doc_in)))
        ]

    to_right, to_left = edge_copies(1, (sp + 1, 0)), edge_copies(0, (sp - 1, 1))

    @pl.when(has_right)
    def _():
        for copy in to_right:
            copy.start()

    @pl.when(has_left)
    def _():
        for copy in to_left:
            copy.start()

    span = rows + 16
    swaps = [
        remote(src, dst, swap_send.at[i], swap_recv.at[i], (sp, other))
        for i, (src, dst) in enumerate(
            (
                (product.at[pl.ds(pl.multiple_of(other * (rows - 16), 16), span)], product_in),
                (outer.at[pl.ds(pl.multiple_of(other * rows, rows), rows)], outer_in),
                (taps, taps_in),
            )
        )
    ]
    for copy in swaps:
        copy.start()

    metas = []
    for d in range(1, planes):
        there = place((z + d) % planes * per_plane + p)
        metas.append(remote(meta.at[z], meta.at[z], meta_send.at[d - 1], meta_recv.at[z], there))
    for copy in metas:
        copy.start()

    before = (
        lax.broadcasted_iota(jnp.int32, (rows, rows), 0)
        < lax.broadcasted_iota(jnp.int32, (rows, rows), 1)
    ).astype(F32).astype(BF16)
    rank_of = lax.broadcasted_iota(jnp.int32, (per_plane, cap, rows), 1).astype(F32)
    expert = (
        lax.broadcasted_iota(jnp.int32, (per_plane, rows), 0) + z * per_plane
    ).astype(F32)

    def slots(i):
        table = meta[order[i]]
        hits = [(table[k : k + 1] == expert).astype(F32) for k in range(top)]
        named = sum(hits)
        ahead = dot(named.astype(BF16), before)

        def spread(hit):
            at = jnp.where(hit > 0, ahead, -1.0)
            grid = jnp.broadcast_to(at[:, None, :], (per_plane, cap, rows))
            return jnp.where(grid == rank_of, 1.0, 0.0).reshape(per_plane * cap, rows)

        return named, hits, spread

    def to_slots(i):
        named, _, spread = slots(i)
        return spread(named).astype(BF16)

    def from_slots(i):
        _, hits, spread = slots(i)
        return [jnp.transpose(spread(hit)).astype(BF16) for hit in hits]

    def gate_columns(i):
        table = meta[order[i]]
        return [
            jnp.transpose(jnp.broadcast_to(table[top + k : top + k + 1], (rows, rows)))[:, :1]
            for k in range(top)
        ]

    picks = [to_slots(0)]

    row_at = lax.broadcasted_iota(jnp.int32, (rows, chan), 0)
    prod = product[pl.ds(pl.multiple_of(tp * rows, rows), rows)].astype(F32)
    seam = [product[rows - 16 : rows].astype(F32)[15:], product[rows : rows + 16].astype(F32)[:1]]
    for copy in swaps:
        copy.wait_recv()
    prod_in = product_in[pl.ds(pl.multiple_of(tp * 16, 16), rows)].astype(F32)
    seam_in = [product_in[:16].astype(F32)[15:], product_in[rows:].astype(F32)[:1]]

    doc = jnp.broadcast_to(docs[...], (8, length))
    lane = lax.broadcasted_iota(jnp.int32, (8, length), 1)
    same_prev = jnp.where((pltpu.roll(doc, 1, axis=1) == doc) & (lane > 0), 1.0, 0.0)
    same_next = jnp.where(
        (pltpu.roll(doc, length - 1, axis=1) == doc) & (lane < length - 1), 1.0, 0.0
    )

    def column(row):
        mine = jnp.where(tp == 0, row[:1, :rows], row[:1, rows:])
        return jnp.transpose(jnp.broadcast_to(mine, (128, rows)))[:, :1]

    before_col, after_col = column(same_prev), column(same_next)

    def convolve(values_f, ends, weights):
        prev = jnp.where(row_at == 0, ends[0], pltpu.roll(values_f, 1, axis=0))
        nxt = jnp.where(row_at == rows - 1, ends[1], pltpu.roll(values_f, rows - 1, axis=0))
        return (
            weights[0:1] * prev * before_col
            + weights[1:2] * values_f
            + weights[2:3] * nxt * after_col
        )

    halves = [
        (
            convolve(prod, seam, taps[...]), taps,
            outer[pl.ds(pl.multiple_of(tp * rows, rows), rows)].astype(F32), tp,
        ),
        (convolve(prod_in, seam_in, taps_in[...]), taps_in, outer_in[...].astype(F32), other),
    ]
    mixed = [(gate * conv).astype(BF16) for conv, _, gate, _ in halves]
    for load in loads[8:11]:
        load.wait()

    def project(pieces, c):
        return sum(
            dot(
                rows_of,
                ow[pl.ds(pl.multiple_of(half[3] * chan, chan), chan), c * tile : (c + 1) * tile],
            )
            for rows_of, half in zip(pieces, halves)
        )

    squares = jnp.zeros((rows, 1), F32)
    for c in range(PARTS):
        part = stream[:, c * tile : (c + 1) * tile].astype(F32) + project(mixed, c)
        resid[c] = part
        squares = squares + jnp.sum(part * part, axis=1, keepdims=True)
    scale = lax.rsqrt(squares / width + 1e-06)

    def first_rows(x):
        return jnp.where(tp == 0, x[:16], x[rows - 16 :])

    late = pl.ds(pl.multiple_of(tp * (rows - 16), 16), 16)
    early = pl.ds(pl.multiple_of(other * 16, 16), rows - 16)

    def piece(j, n):
        if n == PARTS:
            return block.at[j, pl.ds(0, 2), late]
        return block.at[j, n, early] if n < 2 else block.at[j, n]

    def hop(j, n, sem, device):
        return remote(piece(j, n), piece(j, n), sem, hop_recv.at[j, n], device)

    def own_start(n):
        @pl.when(is_middle)
        def _():
            hop(z, n, out_send, outward).start()

        if n < 2 or n == PARTS:
            hop(z, n, in_send, inward).start()
        else:

            @pl.when(is_end)
            def _():
                hop(z, n, in_send, inward).start()

    def arrived(i, n):
        wait_for(piece(order[i], n), hop_recv.at[order[i], n])

    def forward(i, n):
        arrived(i, n)
        if i == 1:
            hop(order[1], n, in_send, inward).start()
        else:
            hop(order[i], n, out_send, outward).start()

    peers = [
        (p // 4 + k // 4) % 2 * 4 + (p // 2 + k // 2) % 2 * 2 + (p + k) % 2
        for k in range(per_plane - 1, 0, -1)
    ]

    def group(src, dst, source_sem, target_sem):
        for peer in peers:
            remote(
                src.at[peer], dst.at[p], source_sem, target_sem, place(z * per_plane + peer)
            ).start()

    def wait_group(buf, sem):
        wait_for(buf.at[pl.ds(0, per_plane - 1)], sem)

    def dispatch(i, c):
        if i > 0 and not relaying[0]:
            arrived(i, c)
            if c == 0:
                arrived(i, PARTS)
        send[i, c] = (
            dot(picks[i], block[order[i], c]).astype(BF16).reshape(per_plane, cap, tile)
        )
        group(send.at[i, c], recv.at[i, c], disp_send, disp_recv.at[i, c])
        recv[i, c, p] = send[i, c, p]

    def upward(i, c):
        wait_group(recv.at[i, c], disp_recv.at[i, c])
        x = recv[i, c].reshape(per_plane * cap, tile)
        for f in range(0, ff, 256):
            a = dot(x, wg[c * tile : (c + 1) * tile, f : f + 256])
            b = dot(x, wu[c * tile : (c + 1) * tile, f : f + 256])
            if c > 0:
                a = acc_gate[:, f : f + 256] + a
                b = acc_up[:, f : f + 256] + b
            if c < PARTS - 1:
                acc_gate[:, f : f + 256] = a
                acc_up[:, f : f + 256] = b
            else:
                hidden[:, f : f + 256] = (a / (1.0 + jnp.exp(-a)) * b).astype(BF16)

    def hand_back(i, c):
        group(outb.at[i, c], ret.at[i, c], back_send, back_recv.at[i, c])

    def downward(i, c, sends):
        outb[i, c] = (
            dot(hidden[...], wd[:, c * tile : (c + 1) * tile])
            .astype(BF16)
            .reshape(per_plane, cap, tile)
        )
        if sends:
            hand_back(i, c)
        ret[i, c, p] = outb[i, c, p]

    spread_back, relaying = {}, [False]

    def part_copy(i, c, slot, device):
        return remote(
            part_out.at[i - 1, c], part_in.at[slot, c],
            part_send, part_recv.at[slot, c], device,
        )

    def combine(i, c):
        if i not in spread_back:
            spread_back[i] = (from_slots(i), gate_columns(i))
        wait_group(ret.at[i, c], back_recv.at[i, c])
        given = ret[i, c].reshape(per_plane * cap, tile)
        part = sum(gate * dot(pick, given) for pick, gate in zip(*spread_back[i]))
        if i == 0:
            resid[c] += part
            return

        if relaying[0]:
            local[i - 1, c] = part
        else:
            part_out[i - 1, c] = part.astype(BF16)
            part_copy(i, c, planes if i == 1 else order[i], inward).start()

    def relay(i, c):
        wait_for(part_in.at[order[i], c], part_recv.at[order[i], c])
        part_out[i - 1, c] = (local[i - 1, c] + part_in[order[i], c].astype(F32)).astype(BF16)
        part_copy(i, c, order[i], outward if i == 1 else inward).start()

    def finish(c, both):
        part = resid[c]
        if both:
            wait_for(part_in.at[planes, c], part_recv.at[planes, c])
            part = part + part_in[planes, c].astype(F32)
        wait_for(part_in.at[z, c], part_recv.at[z, c])
        out[:, c * tile : (c + 1) * tile] = (part + part_in[z, c].astype(F32)).astype(BF16)

    def normed(part, by, c):
        return (part * by * gain[:, c * tile : (c + 1) * tile]).astype(BF16)

    for c in range(PARTS):
        block[z, c] = normed(resid[c], scale, c)
        if c < 2:
            own_start(c)

    @pl.when(((tp == 0) & has_left) | ((tp == 1) & has_right))
    def _():
        for q in range(tp_size):
            wait_for(edge_in.at[q], edge_recv.at[q, 0])
            wait_for(doc_in.at[q], edge_recv.at[q, 1])

    ours = jnp.where(tp == 0, docs[:, :1], docs[:, length - 1 :])
    beyond = jnp.where(tp == 0, doc_in[0][:, length - 1 :], doc_in[0][:, :1])
    inside = jnp.where(tp == 0, sp > 0, sp < sp_size - 1)
    joined = jnp.where((ours == beyond) & inside, 1.0, 0.0)
    at_edge = lax.broadcasted_iota(jnp.int32, (16, chan), 0) == tp * 15
    fixed = []
    for conv, weights, gate, half in halves:
        edge = edge_in[half].astype(F32)
        term = (
            jnp.where(tp == 0, weights[0:1], weights[2:3])
            * jnp.where(tp == 0, edge[15:], edge[:1])
            * joined
        )
        fixed.append(
            (first_rows(gate) * (first_rows(conv) + jnp.where(at_edge, term, 0.0))).astype(BF16)
        )
    squares = jnp.zeros((16, 1), F32)
    parts = []
    for c in range(PARTS):
        part = stream[late, c * tile : (c + 1) * tile].astype(F32) + project(fixed, c)
        resid[c, late] = part
        parts.append(part)
        squares = squares + jnp.sum(part * part, axis=1, keepdims=True)
    late_scale = lax.rsqrt(squares / width + 1e-06)
    for c in range(PARTS):
        block[z, c, late] = normed(parts[c], late_scale, c)
        if c > 0:
            own_start(c if c > 1 else PARTS)
    for c in range(PARTS):
        dispatch(0, c)

    for i in range(1, planes):
        wait_for(meta.at[order[i]], meta_recv.at[order[i]])
    for load in loads[11:13]:
        load.wait()

    def own_rest():
        for c in range(2, PARTS):
            hop(z, c, in_send, inward).start()

    def run(plan, relays):
        relaying[0] = relays
        picks[1:] = []
        spread_back.clear()
        steps = {
            "U": upward, "D": dispatch, "F": forward, "C": combine, "R": relay,
            "E": lambda i, c: finish(c, i == 1),
            "N": lambda i, c: downward(i, c, True),
            "K": lambda i, c: downward(i, c, False),
            "S": hand_back,
            "P": lambda i, c: picks.append(to_slots(i)),
            "W": lambda i, c: loads[13].wait(),
            "O": lambda i, c: own_rest(),
        }
        for name in " ".join(plan).split():
            steps[name[0]](int(name[1]), int(name[2]))

    @pl.when(is_end)
    def _():
        run(
            (
                "U00 P10 D10 D11", "U01 D12 U02 U03", "W00 K00 K01 K02", "K03 D13 S00 S01",
                "U10 U11 U12 U13", "N10 N11 P20 D20", "D21 C10 D22 N12", "C11 D23 N13 U20",
                "U21 C12 U22 P30", "U23 N20 D30 D31", "C13 N21 D32 C20", "N22 D33 N23 C21",
                "U30 U31 C22 U32", "U33 N30 N31 N32", "N33 S02 S03 C23", "C30 C31 C32 C33",
                "C00 C01 C02 C03", "E00 E01 E02 E03",
            ),
            False,
        )

    @pl.when(is_middle)
    def _():
        run(
            (
                "P10 F10 U00 F11", "F14 D10 D11 U01", "U02 F20 F12 D12", "P20 U03 W00 K00",
                "K01 K02 K03 F21", "F24 D20 D21 F13", "O00 D13 U10 U11", "F22 D22 U12 F23",
                "D23 U13 N10 N11", "N12 N13 F30 F31", "F34 U20 U21 U22", "U23 N20 N21 N22",
                "N23 F32 F33 P30", "D30 D31 D32 D33", "C10 C11 C12 C13", "C20 C21 U30 U31",
                "C22 C23 U32 U33", "N30 N31 N32 N33", "R20 R21 S00 S01", "S02 S03 R22 C30",
                "R10 C31 R23 C32", "R11 C33 R12 C00", "R30 R13 C01 R31", "C02 R32 C03 E10",
                "R33 E11 E12 E13",
            ),
            True,
        )

    for copy in metas + swaps:
        copy.wait_send()

    @pl.when(has_right)
    def _():
        for copy in to_right:
            copy.wait_send()

    @pl.when(has_left)
    def _():
        for copy in to_left:
            copy.wait_send()

    most = pl.ds(0, per_plane - 1)
    wait_for(send.at[:, :, most], disp_send)
    wait_for(outb.at[:, :, most], back_send)
    wait_for(part_out, part_send)

    @pl.when(is_end)
    def _():
        wait_for(block.at[0], in_send)

    @pl.when(is_middle)
    def _():
        wait_for(block.at[pl.ds(0, 2)], in_send)
        wait_for(block.at[pl.ds(0, 3)], out_send)


def fused(
    tp_size, planes, per_plane, cap,
    stream, outer_gate, inner_gate, conv_values, doc_ids, conv_taps, out_weight, norm_gain,
    route_ids, route_logits, group_weight, w_gate, w_up, w_down,
):
    rows, width = stream.shape
    length, chan = inner_gate.shape
    ff, top = w_gate.shape[2], route_ids.shape[1]
    tile = width // PARTS
    slotted = pltpu.VMEM((planes, PARTS, per_plane, cap, tile), BF16)
    dma = pltpu.SemaphoreType.DMA
    return pl.pallas_call(
        functools.partial(fused_kernel, tp_size, planes, per_plane, cap),
        out_shape=jax.ShapeDtypeStruct((rows, width), BF16),
        in_specs=[pl.BlockSpec(memory_space=pltpu.HBM)] * 14,
        out_specs=pl.BlockSpec(memory_space=pltpu.VMEM),
        scratch_shapes=[
            pltpu.VMEM((length, chan), BF16),
            pltpu.VMEM((length, chan), BF16),
            pltpu.VMEM((top, rows), jnp.int32),
            pltpu.VMEM((top, rows), F32),
            pltpu.VMEM((1, rows), F32),
            pltpu.VMEM((1, length), jnp.int32),
            pltpu.VMEM(conv_taps.shape, F32),
            pltpu.VMEM((length, chan), BF16),
            pltpu.VMEM((1, width), F32),
            pltpu.VMEM((rows, width), BF16),
            pltpu.VMEM(out_weight.shape, BF16),
            pltpu.VMEM((width, ff), BF16),
            pltpu.VMEM((width, ff), BF16),
            pltpu.VMEM((ff, width), BF16),
            pltpu.VMEM((length, chan), BF16),
            pltpu.VMEM((rows + 16, chan), BF16),
            pltpu.VMEM((rows, chan), BF16),
            pltpu.VMEM(conv_taps.shape, F32),
            pltpu.VMEM((2, 16, chan), BF16),
            pltpu.VMEM((2, 16, chan), BF16),
            pltpu.VMEM((2, 1, length), jnp.int32),
            pltpu.VMEM((PARTS, rows, tile), F32),
            pltpu.VMEM((planes, 8, rows), F32),
            pltpu.VMEM((planes, PARTS, rows, tile), BF16),
            slotted, slotted, slotted, slotted,
            pltpu.VMEM((per_plane * cap, ff), F32),
            pltpu.VMEM((per_plane * cap, ff), F32),
            pltpu.VMEM((per_plane * cap, ff), BF16),
            pltpu.VMEM((planes - 1, PARTS, rows, tile), F32),
            pltpu.VMEM((planes - 1, PARTS, rows, tile), BF16),
            pltpu.VMEM((planes + 1, PARTS, rows, tile), BF16),
            dma((14,)), dma((4,)), dma((2, 2)), dma((3,)), dma((3,)), dma((planes - 1,)), dma((planes,)),
            dma, dma, dma((planes, PARTS + 1)), dma, dma((planes, PARTS)), dma, dma((planes, PARTS)),
            dma, dma((planes + 1, PARTS)),
        ],
        compiler_params=pltpu.CompilerParams(
            collective_id=0, has_side_effects=True, vmem_limit_bytes=48 * 1024 * 1024
        ),
    )(
        *[
            pltpu.with_memory_space_constraint(x, pltpu.HBM)
            for x in (
                inner_gate, conv_values, route_ids.T, route_logits.T, group_weight[None, :],
                doc_ids[None, :], conv_taps, outer_gate, norm_gain[None, :], stream,
                out_weight, w_gate, w_up, w_down,
            )
        ]
    )


def body(*args):
    stream, route_ids = args[0], args[8]
    tp_size = lax.axis_size("tp")
    total = lax.axis_size("sp") * tp_size
    top = route_ids.shape[1]
    cap = 2 * stream.shape[0] * top // total
    planes = 4
    per_plane = total // planes
    if tp_size != 2 or top != 2 or per_plane != 8 or total % planes or cap % 16 or per_plane * cap != stream.shape[0]:
        return on_device(*args)
    return fused(tp_size, planes, per_plane, cap, *args)


def solution(mesh):
    placed = (
        P(("sp", "tp"), None),
        P("sp", "tp"),
        P("sp", "tp"),
        P("sp", "tp"),
        P("sp"),
        P(None, "tp"),
        P(),
        P(),
        P(("sp", "tp"), None),
        P(("sp", "tp"), None),
        P(("sp", "tp")),
        P(("sp", "tp"), None, None),
        P(("sp", "tp"), None, None),
        P(("sp", "tp"), None, None),
    )
    return jax.shard_map(
        body, mesh=mesh, in_specs=placed, out_specs=P(("sp", "tp"), None), check_vma=False
    )
```

```python
import functools

import jax
import jax.numpy as jnp
from jax import lax
from jax.experimental import pallas as pl
from jax.experimental.pallas import tpu as pltpu
from jax.sharding import PartitionSpec as P


def padded_2(shard, sides, width):
    for axis, dim in sides:
        size, length = (lax.axis_size(axis), shard.shape[dim])
        up = [(i, (i + 1) % size) for i in range(size - 1)]
        down = [(j, i) for i, j in up]
        last = lax.slice_in_dim(shard, length - width, length, axis=dim)
        leading = lax.slice_in_dim(shard, 0, width, axis=dim)
        before = lax.ppermute(last, axis, up)
        after = lax.ppermute(leading, axis, down)
        shard = jnp.concatenate([before, shard, after], axis=dim)
    return shard


def on_device(
    stream,
    outer_gate,
    inner_gate,
    conv_values,
    doc_ids,
    conv_taps,
    out_weight,
    norm_gain,
    route_ids,
    route_logits,
    group_weight,
    w_gate,
    w_up,
    w_down,
):
    tok_rows = stream.shape[0]
    width = stream.shape[1]
    product = (inner_gate.astype(jnp.float32) * conv_values.astype(jnp.float32)).astype(
        jnp.bfloat16
    )
    doc_float = doc_ids.astype(jnp.bfloat16)
    padded, padded_docs = (padded_2(product, (("sp", 0),), 1), padded_2(doc_float, (("sp", 0),), 1))
    same_prev = (padded_docs[:-2] == doc_float).astype(jnp.float32)[:, None]
    same_next = (padded_docs[2:] == doc_float).astype(jnp.float32)[:, None]
    conv = (
        conv_taps[0] * padded[:-2].astype(jnp.float32) * same_prev
        + conv_taps[1] * product.astype(jnp.float32)
        + conv_taps[2] * padded[2:].astype(jnp.float32) * same_next
    )
    mixed = (outer_gate.astype(jnp.float32) * conv).astype(jnp.bfloat16)
    channels = lax.all_to_all(mixed, "tp", split_axis=0, concat_axis=1, tiled=True)
    projected = jnp.dot(channels, out_weight, preferred_element_type=jnp.float32)
    resid = stream.astype(jnp.float32) + projected
    scale = lax.rsqrt(jnp.mean(resid * resid, axis=-1, keepdims=True) + 1e-06)
    normed = (resid * scale * norm_gain).astype(jnp.bfloat16)
    expert_total = lax.axis_size("sp") * lax.axis_size("tp")
    top_count = route_ids.shape[1]
    capacity = 2 * tok_rows * top_count // expert_total
    flat_ids = route_ids.reshape(-1)
    one_hot = (flat_ids[:, None] == jnp.arange(expert_total, dtype=jnp.int32)[None, :]).astype(
        jnp.int32
    )
    rank = jnp.sum((jnp.cumsum(one_hot, axis=0) - 1) * one_hot, axis=1)
    slot = flat_ids * capacity + rank
    slot_count = expert_total * capacity
    source_row = (
        jnp.zeros((slot_count,), jnp.int32)
        .at[slot]
        .set(jnp.arange(flat_ids.shape[0], dtype=jnp.int32) // top_count)
    )
    filled = jnp.zeros((slot_count,), jnp.bool_).at[slot].set(True)
    outgoing = jnp.where(filled[:, None], normed[source_row], jnp.zeros((), jnp.bfloat16)).reshape(
        expert_total, capacity, width
    )
    arrived = lax.all_to_all(outgoing, ("sp", "tp"), split_axis=0, concat_axis=0, tiled=True)
    sources, items, features = arrived.shape
    rows_in = arrived.reshape(sources * items, features)
    hidden = (
        jax.nn.silu(jnp.dot(rows_in, w_gate[0], preferred_element_type=jnp.float32))
        * jnp.dot(rows_in, w_up[0], preferred_element_type=jnp.float32)
    ).astype(jnp.bfloat16)
    outputs = jnp.dot(hidden, w_down[0], preferred_element_type=jnp.float32).astype(jnp.bfloat16)
    returned = lax.all_to_all(
        outputs.reshape(sources, items, features),
        ("sp", "tp"),
        split_axis=0,
        concat_axis=0,
        tiled=True,
    )
    picked = (
        returned.reshape(slot_count, width)[slot]
        .astype(jnp.float32)
        .reshape(tok_rows, top_count, width)
    )
    expo = jnp.exp(route_logits)
    gate = group_weight[:, None] * expo / jnp.sum(expo, axis=1, keepdims=True)
    result = resid + jnp.sum(gate[:, :, None] * picked, axis=1)
    return result.astype(jnp.bfloat16)


MESH = pl.DeviceIdType.MESH
F32, BF16 = jnp.float32, jnp.bfloat16


def dot(a, b):
    return jnp.dot(a, b, preferred_element_type=F32)


PARTS = 4


def fused_kernel(
    tp_size, planes, per_plane, cap,
    inner_hbm, values_hbm, ids_hbm, logits_hbm, weight_hbm, docs_hbm, taps_hbm, outer_hbm,
    gain_hbm, stream_hbm, ow_hbm, wg_hbm, wu_hbm, wd_hbm,
    out,
    inner, values, ids, logits, weight, docs, taps, outer, gain, stream, ow, wg, wu, wd,
    product, product_in, outer_in, taps_in, edge_out, edge_in, doc_in, resid,
    meta, block, send, recv, outb, ret, acc_gate, acc_up, hidden, local, part_out, part_in,
    load_sem, edge_send, edge_recv, swap_send, swap_recv, meta_send, meta_recv,
    in_send, out_send, hop_recv, disp_send, disp_recv, back_send, back_recv,
    part_send, part_recv,
):
    sp, tp = lax.axis_index("sp"), lax.axis_index("tp")
    sp_size = planes * per_plane // tp_size
    total = planes * per_plane
    me = sp * tp_size + tp
    z, p = me // per_plane, me % per_plane
    rows, width = stream.shape
    length, chan = inner.shape
    tile = width // PARTS
    top = ids.shape[0]
    ff = hidden.shape[1]
    other = 1 - tp

    middle = (z % 3 + 1) // 2
    is_middle, is_end = middle == 1, middle == 0
    step = 1 - 2 * (z // 2)
    order = [z, z + step * (1 - 2 * middle), z + step * (3 - middle), z + step * (2 - middle)]

    def place(index):
        return (index // tp_size, index % tp_size)

    inward = place((z + step) * per_plane + p)
    outward = place((z - step) * per_plane + p)

    def remote(src, dst, source_sem, target_sem, device):
        return pltpu.make_async_remote_copy(
            src_ref=src, dst_ref=dst, send_sem=source_sem, recv_sem=target_sem,
            device_id=device, device_id_type=MESH,
        )

    def wait_for(ref, sem):
        pltpu.make_async_copy(ref, ref, sem).wait()

    loads = [
        pltpu.make_async_copy(src, dst, load_sem.at[i])
        for i, (src, dst) in enumerate(
            (
                (inner_hbm, inner), (values_hbm, values), (ids_hbm, ids), (logits_hbm, logits),
                (weight_hbm, weight), (docs_hbm, docs), (taps_hbm, taps), (outer_hbm, outer),
                (gain_hbm, gain), (stream_hbm, stream), (ow_hbm, ow),
                (wg_hbm.at[0], wg), (wu_hbm.at[0], wu), (wd_hbm.at[0], wd),
            )
        )
    ]
    for load in loads:
        load.start()

    has_left, has_right = sp > 0, sp < sp_size - 1
    barrier = pltpu.get_barrier_semaphore()

    def greet(device):
        pl.semaphore_signal(barrier, inc=1, device_id=device, device_id_type=MESH)

    @pl.when((tp == 0) & has_left)
    def _():
        for q in range(tp_size):
            greet((sp - 1, q))

    @pl.when((tp == 1) & has_right)
    def _():
        for q in range(tp_size):
            greet((sp + 1, q))

    for d in range(1, planes):
        greet(place((z + d) % planes * per_plane + p))
    for d in range(1, per_plane):
        greet(place(z * per_plane + (p + d) % per_plane))

    @pl.when(((tp == 0) & (sp == 0)) | ((tp == 1) & (sp == sp_size - 1)))
    def _():
        edge_in[...] = jnp.zeros_like(edge_in)
        doc_in[...] = jnp.zeros_like(doc_in)

    for load in loads[:2]:
        load.wait()
    product[...] = (inner[...].astype(F32) * values[...].astype(F32)).astype(BF16)
    edge_out[0] = product[:16]
    edge_out[1] = product[length - 16 :]
    for load in loads[2:8]:
        load.wait()
    expo = jnp.exp(logits[...])
    gates = weight[...] * expo / jnp.sum(expo, axis=0, keepdims=True)
    meta[z] = jnp.concatenate([ids[...].astype(F32), gates, ids[...].astype(F32), gates], axis=0)
    pl.semaphore_wait(
        barrier,
        planes + per_plane - 2 + (sp + sp_size - 1) // sp_size + (2 * sp_size - 2 - sp) // sp_size,
    )

    def edge_copies(side, device):
        return [
            remote(
                source, target.at[tp], edge_send.at[2 * side + kind], edge_recv.at[tp, kind], device
            )
            for kind, (source, target) in enumerate(((edge_out.at[side], edge_in), (docs, doc_in)))
        ]

    to_right, to_left = edge_copies(1, (sp + 1, 0)), edge_copies(0, (sp - 1, 1))

    @pl.when(has_right)
    def _():
        for copy in to_right:
            copy.start()

    @pl.when(has_left)
    def _():
        for copy in to_left:
            copy.start()

    span = rows + 16
    swaps = [
        remote(src, dst, swap_send.at[i], swap_recv.at[i], (sp, other))
        for i, (src, dst) in enumerate(
            (
                (product.at[pl.ds(pl.multiple_of(other * (rows - 16), 16), span)], product_in),
                (outer.at[pl.ds(pl.multiple_of(other * rows, rows), rows)], outer_in),
                (taps, taps_in),
            )
        )
    ]
    for copy in swaps:
        copy.start()

    metas = []
    for d in range(1, planes):
        there = place((z + d) % planes * per_plane + p)
        metas.append(remote(meta.at[z], meta.at[z], meta_send.at[d - 1], meta_recv.at[z], there))
    for copy in metas:
        copy.start()

    before = (
        lax.broadcasted_iota(jnp.int32, (rows, rows), 0)
        < lax.broadcasted_iota(jnp.int32, (rows, rows), 1)
    ).astype(F32).astype(BF16)
    rank_of = lax.broadcasted_iota(jnp.int32, (per_plane, cap, rows), 1).astype(F32)
    expert = (
        lax.broadcasted_iota(jnp.int32, (per_plane, rows), 0) + z * per_plane
    ).astype(F32)

    def slots(i):
        table = meta[order[i]]
        hits = [(table[k : k + 1] == expert).astype(F32) for k in range(top)]
        named = sum(hits)
        ahead = dot(named.astype(BF16), before)

        def spread(hit):
            at = jnp.where(hit > 0, ahead, -1.0)
            grid = jnp.broadcast_to(at[:, None, :], (per_plane, cap, rows))
            return jnp.where(grid == rank_of, 1.0, 0.0).reshape(per_plane * cap, rows)

        return named, hits, spread

    def to_slots(i):
        named, _, spread = slots(i)
        return spread(named).astype(BF16)

    def from_slots(i):
        _, hits, spread = slots(i)
        return [jnp.transpose(spread(hit)).astype(BF16) for hit in hits]

    def gate_columns(i):
        table = meta[order[i]]
        return [
            jnp.transpose(jnp.broadcast_to(table[top + k : top + k + 1], (rows, rows)))[:, :1]
            for k in range(top)
        ]

    picks = [to_slots(0)]

    row_at = lax.broadcasted_iota(jnp.int32, (rows, chan), 0)
    prod = product[pl.ds(pl.multiple_of(tp * rows, rows), rows)].astype(F32)
    seam = [product[rows - 16 : rows].astype(F32)[15:], product[rows : rows + 16].astype(F32)[:1]]
    for copy in swaps:
        copy.wait_recv()
    prod_in = product_in[pl.ds(pl.multiple_of(tp * 16, 16), rows)].astype(F32)
    seam_in = [product_in[:16].astype(F32)[15:], product_in[rows:].astype(F32)[:1]]

    doc = jnp.broadcast_to(docs[...], (8, length))
    lane = lax.broadcasted_iota(jnp.int32, (8, length), 1)
    same_prev = jnp.where((pltpu.roll(doc, 1, axis=1) == doc) & (lane > 0), 1.0, 0.0)
    same_next = jnp.where(
        (pltpu.roll(doc, length - 1, axis=1) == doc) & (lane < length - 1), 1.0, 0.0
    )

    def column(row):
        mine = jnp.where(tp == 0, row[:1, :rows], row[:1, rows:])
        return jnp.transpose(jnp.broadcast_to(mine, (128, rows)))[:, :1]

    before_col, after_col = column(same_prev), column(same_next)

    def convolve(values_f, ends, weights):
        prev = jnp.where(row_at == 0, ends[0], pltpu.roll(values_f, 1, axis=0))
        nxt = jnp.where(row_at == rows - 1, ends[1], pltpu.roll(values_f, rows - 1, axis=0))
        return (
            weights[0:1] * prev * before_col
            + weights[1:2] * values_f
            + weights[2:3] * nxt * after_col
        )

    halves = [
        (
            convolve(prod, seam, taps[...]), taps,
            outer[pl.ds(pl.multiple_of(tp * rows, rows), rows)].astype(F32), tp,
        ),
        (convolve(prod_in, seam_in, taps_in[...]), taps_in, outer_in[...].astype(F32), other),
    ]
    mixed = [(gate * conv).astype(BF16) for conv, _, gate, _ in halves]
    for load in loads[8:11]:
        load.wait()

    def project(pieces, c):
        return sum(
            dot(
                rows_of,
                ow[pl.ds(pl.multiple_of(half[3] * chan, chan), chan), c * tile : (c + 1) * tile],
            )
            for rows_of, half in zip(pieces, halves)
        )

    squares = jnp.zeros((rows, 1), F32)
    for c in range(PARTS):
        part = stream[:, c * tile : (c + 1) * tile].astype(F32) + project(mixed, c)
        resid[c] = part
        squares = squares + jnp.sum(part * part, axis=1, keepdims=True)
    scale = lax.rsqrt(squares / width + 1e-06)

    def first_rows(x):
        return jnp.where(tp == 0, x[:16], x[rows - 16 :])

    late = pl.ds(pl.multiple_of(tp * (rows - 16), 16), 16)
    early = pl.ds(pl.multiple_of(other * 16, 16), rows - 16)

    def piece(j, n):
        if n == PARTS:
            return block.at[j, pl.ds(0, 2), late]
        return block.at[j, n, early] if n < 2 else block.at[j, n]

    def hop(j, n, sem, device):
        return remote(piece(j, n), piece(j, n), sem, hop_recv.at[j, n], device)

    def own_start(n):
        @pl.when(is_middle)
        def _():
            hop(z, n, out_send, outward).start()

        if n < 2 or n == PARTS:
            hop(z, n, in_send, inward).start()
        else:

            @pl.when(is_end)
            def _():
                hop(z, n, in_send, inward).start()

    def arrived(i, n):
        wait_for(piece(order[i], n), hop_recv.at[order[i], n])

    def forward(i, n):
        arrived(i, n)
        if i == 1:
            hop(order[1], n, in_send, inward).start()
        else:
            hop(order[i], n, out_send, outward).start()

    peers = [
        (p // 4 + k // 4) % 2 * 4 + (p // 2 + k // 2) % 2 * 2 + (p + k) % 2
        for k in range(per_plane - 1, 0, -1)
    ]

    def group(src, dst, source_sem, target_sem):
        for peer in peers:
            remote(
                src.at[peer], dst.at[p], source_sem, target_sem, place(z * per_plane + peer)
            ).start()

    def wait_group(buf, sem):
        wait_for(buf.at[pl.ds(0, per_plane - 1)], sem)

    def dispatch(i, c):
        if i > 0 and not relaying[0]:
            arrived(i, c)
            if c == 0:
                arrived(i, PARTS)
        send[i, c] = (
            dot(picks[i], block[order[i], c]).astype(BF16).reshape(per_plane, cap, tile)
        )
        group(send.at[i, c], recv.at[i, c], disp_send, disp_recv.at[i, c])
        recv[i, c, p] = send[i, c, p]

    def upward(i, c):
        wait_group(recv.at[i, c], disp_recv.at[i, c])
        x = recv[i, c].reshape(per_plane * cap, tile)
        for f in range(0, ff, 256):
            a = dot(x, wg[c * tile : (c + 1) * tile, f : f + 256])
            b = dot(x, wu[c * tile : (c + 1) * tile, f : f + 256])
            if c > 0:
                a = acc_gate[:, f : f + 256] + a
                b = acc_up[:, f : f + 256] + b
            if c < PARTS - 1:
                acc_gate[:, f : f + 256] = a
                acc_up[:, f : f + 256] = b
            else:
                hidden[:, f : f + 256] = (a / (1.0 + jnp.exp(-a)) * b).astype(BF16)

    def hand_back(i, c):
        group(outb.at[i, c], ret.at[i, c], back_send, back_recv.at[i, c])

    def downward(i, c, sends):
        outb[i, c] = (
            dot(hidden[...], wd[:, c * tile : (c + 1) * tile])
            .astype(BF16)
            .reshape(per_plane, cap, tile)
        )
        if sends:
            hand_back(i, c)
        ret[i, c, p] = outb[i, c, p]

    spread_back, relaying = {}, [False]

    def halves_of(i, c):
        if i == planes - 1 and c == PARTS - 1:
            return [(pl.ds(0, rows // 2), c), (pl.ds(rows // 2, rows // 2), PARTS)]
        return [(pl.ds(0, rows), c)]

    def part_copy(i, c, slot, device, span, sem):
        return remote(
            part_out.at[i - 1, c, span], part_in.at[slot, c, span],
            part_send, part_recv.at[slot, sem], device,
        )

    def combine(i, c):
        if i not in spread_back:
            spread_back[i] = (from_slots(i), gate_columns(i))
        wait_group(ret.at[i, c], back_recv.at[i, c])
        given = ret[i, c].reshape(per_plane * cap, tile)
        part = sum(gate * dot(pick, given) for pick, gate in zip(*spread_back[i]))
        if i == 0:
            resid[c] += part
            return

        if relaying[0]:
            local[i - 1, c] = part
        else:
            part_out[i - 1, c] = part.astype(BF16)
            for span, sem in halves_of(i, c):
                part_copy(i, c, planes if i == 1 else order[i], inward, span, sem).start()

    def relay(i, c):
        for span, sem in halves_of(i, c):
            wait_for(part_in.at[order[i], c, span], part_recv.at[order[i], sem])
            part_out[i - 1, c, span] = (
                local[i - 1, c, span] + part_in[order[i], c, span].astype(F32)
            ).astype(BF16)
            part_copy(i, c, order[i], outward if i == 1 else inward, span, sem).start()

    def finish(c, both):
        part = resid[c]
        if both:
            wait_for(part_in.at[planes, c], part_recv.at[planes, c])
            part = part + part_in[planes, c].astype(F32)
        for span, sem in halves_of(planes - 1 if both else 1, c):
            wait_for(part_in.at[z, c, span], part_recv.at[z, sem])
        out[:, c * tile : (c + 1) * tile] = (part + part_in[z, c].astype(F32)).astype(BF16)

    def normed(part, by, c):
        return (part * by * gain[:, c * tile : (c + 1) * tile]).astype(BF16)

    for c in range(PARTS):
        block[z, c] = normed(resid[c], scale, c)
        if c < 2:
            own_start(c)

    @pl.when(((tp == 0) & has_left) | ((tp == 1) & has_right))
    def _():
        for q in range(tp_size):
            wait_for(edge_in.at[q], edge_recv.at[q, 0])
            wait_for(doc_in.at[q], edge_recv.at[q, 1])

    ours = jnp.where(tp == 0, docs[:, :1], docs[:, length - 1 :])
    beyond = jnp.where(tp == 0, doc_in[0][:, length - 1 :], doc_in[0][:, :1])
    inside = jnp.where(tp == 0, sp > 0, sp < sp_size - 1)
    joined = jnp.where((ours == beyond) & inside, 1.0, 0.0)
    at_edge = lax.broadcasted_iota(jnp.int32, (16, chan), 0) == tp * 15
    fixed = []
    for conv, weights, gate, half in halves:
        edge = edge_in[half].astype(F32)
        term = (
            jnp.where(tp == 0, weights[0:1], weights[2:3])
            * jnp.where(tp == 0, edge[15:], edge[:1])
            * joined
        )
        fixed.append(
            (first_rows(gate) * (first_rows(conv) + jnp.where(at_edge, term, 0.0))).astype(BF16)
        )
    squares = jnp.zeros((16, 1), F32)
    parts = []
    for c in range(PARTS):
        part = stream[late, c * tile : (c + 1) * tile].astype(F32) + project(fixed, c)
        resid[c, late] = part
        parts.append(part)
        squares = squares + jnp.sum(part * part, axis=1, keepdims=True)
    late_scale = lax.rsqrt(squares / width + 1e-06)
    for c in range(PARTS):
        block[z, c, late] = normed(parts[c], late_scale, c)
        if c > 0:
            own_start(c if c > 1 else PARTS)
    for c in range(PARTS):
        dispatch(0, c)

    for i in range(1, planes):
        wait_for(meta.at[order[i]], meta_recv.at[order[i]])
    for load in loads[11:13]:
        load.wait()

    def own_rest():
        for c in range(2, PARTS):
            hop(z, c, in_send, inward).start()

    def run(plan, relays):
        relaying[0] = relays
        picks[1:] = []
        spread_back.clear()
        steps = {
            "U": upward, "D": dispatch, "F": forward, "C": combine, "R": relay,
            "E": lambda i, c: finish(c, i == 1),
            "N": lambda i, c: downward(i, c, True),
            "K": lambda i, c: downward(i, c, False),
            "S": hand_back,
            "P": lambda i, c: picks.append(to_slots(i)),
            "W": lambda i, c: loads[13].wait(),
            "O": lambda i, c: own_rest(),
        }
        for name in " ".join(plan).split():
            steps[name[0]](int(name[1]), int(name[2]))

    @pl.when(is_end)
    def _():
        run(
            (
                "U00 P10 D10 D11", "U01 D12 U02 U03", "W00 K00 K01 K02", "K03 D13 S00 S01",
                "U10 U11 U12 U13", "N10 N11 P20 D20", "D21 C10 D22 C11", "D23 N12 N13 U20",
                "U21 U22 P30 U23", "N20 C12 D30 D31", "N21 C13 D32 N22", "C20 D33 N23 C21",
                "U30 U31 C22 U32", "U33 N30 N31 N32", "N33 S02 S03 C23", "C30 C31 C32 C33",
                "C00 C01 C02 C03", "E00 E01 E02 E03",
            ),
            False,
        )

    @pl.when(is_middle)
    def _():
        run(
            (
                "P10 F10 U00 F11", "F14 D10 D11 U01", "U02 F20 F12 D12", "P20 U03 W00 K00",
                "K01 K02 K03 F21", "F24 D20 D21 F13", "O00 D13 U10 U11", "F22 D22 U12 F23",
                "D23 U13 N10 N11", "N12 N13 F30 F31", "F34 U20 U21 U22", "U23 N20 N21 N22",
                "N23 F32 F33 P30", "D30 D31 D32 D33", "C10 C11 C12 C13", "C20 C21 U30 U31",
                "C22 C23 R20 U32", "U33 N30 N31 N32", "N33 R21 S00 S01", "S02 S03 R22 C30",
                "R10 C31 R23 C32", "R11 C33 R12 C00", "R30 R13 C01 R31", "C02 R32 C03 E10",
                "R33 E11 E12 E13",
            ),
            True,
        )

    for copy in metas + swaps:
        copy.wait_send()

    @pl.when(has_right)
    def _():
        for copy in to_right:
            copy.wait_send()

    @pl.when(has_left)
    def _():
        for copy in to_left:
            copy.wait_send()

    most = pl.ds(0, per_plane - 1)
    wait_for(send.at[:, :, most], disp_send)
    wait_for(outb.at[:, :, most], back_send)
    wait_for(part_out, part_send)

    @pl.when(is_end)
    def _():
        wait_for(block.at[0], in_send)

    @pl.when(is_middle)
    def _():
        wait_for(block.at[pl.ds(0, 2)], in_send)
        wait_for(block.at[pl.ds(0, 3)], out_send)


def fused(
    tp_size, planes, per_plane, cap,
    stream, outer_gate, inner_gate, conv_values, doc_ids, conv_taps, out_weight, norm_gain,
    route_ids, route_logits, group_weight, w_gate, w_up, w_down,
):
    rows, width = stream.shape
    length, chan = inner_gate.shape
    ff, top = w_gate.shape[2], route_ids.shape[1]
    tile = width // PARTS
    slotted = pltpu.VMEM((planes, PARTS, per_plane, cap, tile), BF16)
    dma = pltpu.SemaphoreType.DMA
    return pl.pallas_call(
        functools.partial(fused_kernel, tp_size, planes, per_plane, cap),
        out_shape=jax.ShapeDtypeStruct((rows, width), BF16),
        in_specs=[pl.BlockSpec(memory_space=pltpu.HBM)] * 14,
        out_specs=pl.BlockSpec(memory_space=pltpu.VMEM),
        scratch_shapes=[
            pltpu.VMEM((length, chan), BF16),
            pltpu.VMEM((length, chan), BF16),
            pltpu.VMEM((top, rows), jnp.int32),
            pltpu.VMEM((top, rows), F32),
            pltpu.VMEM((1, rows), F32),
            pltpu.VMEM((1, length), jnp.int32),
            pltpu.VMEM(conv_taps.shape, F32),
            pltpu.VMEM((length, chan), BF16),
            pltpu.VMEM((1, width), F32),
            pltpu.VMEM((rows, width), BF16),
            pltpu.VMEM(out_weight.shape, BF16),
            pltpu.VMEM((width, ff), BF16),
            pltpu.VMEM((width, ff), BF16),
            pltpu.VMEM((ff, width), BF16),
            pltpu.VMEM((length, chan), BF16),
            pltpu.VMEM((rows + 16, chan), BF16),
            pltpu.VMEM((rows, chan), BF16),
            pltpu.VMEM(conv_taps.shape, F32),
            pltpu.VMEM((2, 16, chan), BF16),
            pltpu.VMEM((2, 16, chan), BF16),
            pltpu.VMEM((2, 1, length), jnp.int32),
            pltpu.VMEM((PARTS, rows, tile), F32),
            pltpu.VMEM((planes, 8, rows), F32),
            pltpu.VMEM((planes, PARTS, rows, tile), BF16),
            slotted, slotted, slotted, slotted,
            pltpu.VMEM((per_plane * cap, ff), F32),
            pltpu.VMEM((per_plane * cap, ff), F32),
            pltpu.VMEM((per_plane * cap, ff), BF16),
            pltpu.VMEM((planes - 1, PARTS, rows, tile), F32),
            pltpu.VMEM((planes - 1, PARTS, rows, tile), BF16),
            pltpu.VMEM((planes + 1, PARTS, rows, tile), BF16),
            dma((14,)), dma((4,)), dma((2, 2)), dma((3,)), dma((3,)), dma((planes - 1,)), dma((planes,)),
            dma, dma, dma((planes, PARTS + 1)), dma, dma((planes, PARTS)), dma, dma((planes, PARTS)),
            dma, dma((planes + 1, PARTS + 1)),
        ],
        compiler_params=pltpu.CompilerParams(
            collective_id=0, has_side_effects=True, vmem_limit_bytes=48 * 1024 * 1024
        ),
    )(
        *[
            pltpu.with_memory_space_constraint(x, pltpu.HBM)
            for x in (
                inner_gate, conv_values, route_ids.T, route_logits.T, group_weight[None, :],
                doc_ids[None, :], conv_taps, outer_gate, norm_gain[None, :], stream,
                out_weight, w_gate, w_up, w_down,
            )
        ]
    )


def body(*args):
    stream, route_ids = args[0], args[8]
    tp_size = lax.axis_size("tp")
    total = lax.axis_size("sp") * tp_size
    top = route_ids.shape[1]
    cap = 2 * stream.shape[0] * top // total
    planes = 4
    per_plane = total // planes
    if tp_size != 2 or top != 2 or per_plane != 8 or total % planes or cap % 16 or per_plane * cap != stream.shape[0]:
        return on_device(*args)
    return fused(tp_size, planes, per_plane, cap, *args)


def solution(mesh):
    placed = (
        P(("sp", "tp"), None),
        P("sp", "tp"),
        P("sp", "tp"),
        P("sp", "tp"),
        P("sp"),
        P(None, "tp"),
        P(),
        P(),
        P(("sp", "tp"), None),
        P(("sp", "tp"), None),
        P(("sp", "tp")),
        P(("sp", "tp"), None, None),
        P(("sp", "tp"), None, None),
        P(("sp", "tp"), None, None),
    )
    return jax.shard_map(
        body, mesh=mesh, in_specs=placed, out_specs=P(("sp", "tp"), None), check_vma=False
    )
```
